32 devices in a mesh: sp: 8 (over z, y), tp: 4 (over x, core).
Axes of the slice: x: 2, y: 2, z: 4, core: 2. Of those that a mesh axis runs over, the one named last changes fastest.
Arguments:
- hidden_state: bfloat16 [1024, 2048], P('sp'), may hold values from -125 to 125
- norm_gain: float32 [2048], replicated, may hold values from 0.1 to 1.9
- route_ids: int32 [1024, 2], P('sp'), may hold values from 0 to 7, all different within a row; in each aligned block of 128 rows (0 to 127, 128 to 255, ...) at most 64 rows name the same one
- route_logits: float32 [1024, 2], P('sp'), may hold values from -6 to 6
- cotangent: bfloat16 [1024, 2048], P('sp'), may hold values from -6 to 6
- w_gate: bfloat16 [8, 2048, 1536], P('sp', None, 'tp'), may hold values from -0.125 to 0.125
- w_up: bfloat16 [8, 2048, 1536], P('sp', None, 'tp'), may hold values from -0.125 to 0.125
- w_down: bfloat16 [8, 1536, 2048], P('sp', 'tp'), may hold values from -0.15625 to 0.15625
- w_out: bfloat16 [2048, 1024], P(None, 'tp'), may hold values from -0.1875 to 0.1875
- query_rows: bfloat16 [1024, 512], P('sp', 'tp'), may hold values from -6 to 6
- key_rows: bfloat16 [1024, 512], P('sp', 'tp'), may hold values from -6 to 6
- value_rows: bfloat16 [1024, 1024], P('sp', 'tp'), may hold values from -6 to 6
- log_decay: float32 [1024, 512], P('sp', 'tp'), may hold values from -1.6 to 0
- head_gain: float32 [1024], P('tp'), may hold values from 0.1 to 1.9
Outputs:
- d_w_gate: bfloat16 [8, 2048, 1536], P('sp', None, 'tp')
- d_w_up: bfloat16 [8, 2048, 1536], P('sp', None, 'tp')
- d_w_down: bfloat16 [8, 1536, 2048], P('sp', 'tp')
- d_w_out: float32 [2048, 1024], P('sp', 'tp')
- d_queries: bfloat16 [1024, 512], P('sp', 'tp')
- d_keys: bfloat16 [1024, 512], P('sp', 'tp')
- d_values: bfloat16 [1024, 1024], P('sp', 'tp')
- d_log_decay: float32 [1024, 512], P('sp', 'tp')
The draws below stay inside these ranges and needn't reach their ends.
Inputs may be any that keep to these rules, and one draw needn't show every extreme that they name: `route_ids`: in the rows of one device each expert is named at most 64 times, a bound that some block reaches; the two experts of a position differ.
All inputs are finite; a program needn't handle non-finite values.
Results may differ from the reference program's by a relative error of at most 0.014.
Values may be sent and summed in bfloat16 or wider, within the bound.
A program may use at most 128 MiB of HBM per device.

```python
import math
import jax
import jax.numpy as jnp
import numpy as np
from jax import lax

D = 2048
HEADS = 8
KEY_DIM = 64
VAL_DIM = 128
FFE = 1536
BLOCK = 64
TOK_DEV = 128
HK = 512
HV = 1024
EXPERTS = 8
CAP = 64
SEQUENCE_TOKENS = 1024
N_SP = 8
N_TP = 4


def draw_hidden_state(key, part):
    every_key = jax.random.split(key, 3)
    row_scale = jnp.exp(jax.random.uniform(every_key[0], (SEQUENCE_TOKENS, 1), minval=0.0, maxval=math.log(10.0)))
    col_scale = jnp.exp(jax.random.uniform(every_key[1], (1, D), minval=0.0, maxval=math.log(3.0)))
    base_vals = jnp.clip(jax.random.normal(every_key[2], (SEQUENCE_TOKENS, D)), -4.0, 4.0)
    return (base_vals * row_scale * col_scale).astype(jnp.bfloat16)


def draw_log_decay(key, part):
    every_key = jax.random.split(key, 7)
    entire_width = HEADS * KEY_DIM
    order_heads = jax.random.permutation(every_key[0], HEADS)
    slow_count = HEADS // 2
    slow_head = (order_heads < slow_count).astype(jnp.float32)
    slow_chan = jnp.repeat(slow_head, KEY_DIM)[None, :]
    slow_rate = math.log(10.0) / (3.0 * SEQUENCE_TOKENS) * jnp.exp(jax.random.uniform(every_key[1], (1, entire_width), minval=math.log(0.5), maxval=0.0))
    fast_rate = jnp.exp(jax.random.uniform(every_key[2], (1, entire_width), minval=math.log(0.01), maxval=math.log(1.0 / 30.0)))
    baseline_decay_rate = slow_chan * slow_rate + (1.0 - slow_chan) * fast_rate
    block_multiplier = jnp.exp(jax.random.uniform(every_key[3], (SEQUENCE_TOKENS // TOK_DEV, 1), minval=-math.log(2.0), maxval=math.log(2.0)))
    block_multiplier = jnp.repeat(block_multiplier, TOK_DEV, axis=0)
    element_multiplier = jax.random.uniform(every_key[4], (SEQUENCE_TOKENS, entire_width), minval=0.5, maxval=1.5)
    spike_positions = jax.random.randint(every_key[5], (3,), 0, SEQUENCE_TOKENS)
    spike_length = jax.random.uniform(every_key[6], (3, entire_width), minval=math.log(0.5), maxval=math.log(0.8))
    spike_token_hits = (jnp.arange(SEQUENCE_TOKENS)[:, None] == spike_positions[None, :]).astype(jnp.float32)
    spike_count = jnp.dot(spike_token_hits, spike_length)
    return -(baseline_decay_rate * block_multiplier * element_multiplier) + spike_count


def spiked(result, key, source, target, parts, factor):
    owner, partner = [(jnp.arange(result.shape[axis_at]) // (result.shape[axis_at] // parts)).reshape([-1 if axis == axis_at else 1 for axis in range(result.ndim)]) for axis_at in (source, target)]
    chosen = jax.random.permutation(key, parts)[partner]
    strong = (owner == chosen) | (owner == (partner + parts // 2) % parts)
    return jnp.where(strong, factor * result, result)


def steps_of(stream_key, extent, cuts, low, high):
    level = 1.0
    for position, blocks in cuts:
        steps = jax.random.uniform(jax.random.fold_in(jax.random.fold_in(stream_key, 6), position), (blocks,), jnp.float32, low / len(cuts), high / len(cuts))
        level = level * jnp.repeat(jnp.exp(steps), extent[position] // blocks).reshape((-1,) + (1,) * (len(extent) - 1 - position))
    return level


def deal_out(stream_key, own, number, rows, number_of, top, limit, slope):
    ranking = jax.random.permutation(stream_key, number_of)
    heavy_load, ordinary = shares(number_of, rows * top, limit, slope, True), shares(number_of, rows * top, limit, slope, False)
    places = jnp.arange(number_of)

    def named(lengths, offset_by):
        used = int((lengths > 0).sum())
        fixed = max(1, used // 4)
        shifted = fixed + (places - fixed + offset_by * (used - fixed)) % max(1, number_of - fixed)
        return jnp.zeros((number_of,), jnp.int32).at[ranking[jnp.where(places < fixed, places, shifted)]].set(jnp.asarray(lengths, jnp.int32))

    lengths = jnp.where(number % 4 == 0, named(heavy_load, number // 4), named(ordinary, number - number // 4 - 1))
    mixed = jax.random.permutation(jax.random.fold_in(own, 3), number_of)
    donor, taker = mixed[0:number_of // 2 * 2:2], mixed[1:number_of // 2 * 2:2]
    room = jnp.minimum(lengths[donor] - 1, limit - lengths[taker]) // 2
    room = jnp.where((donor == ranking[0]) | (taker == ranking[0]) | (lengths[taker] == 0), 0, jnp.maximum(room, 0))
    shifted = jax.random.randint(jax.random.fold_in(own, 4), (number_of // 2,), 0, 1 << 20) % (room + 1)
    lengths = lengths.at[donor].add(-shifted).at[taker].add(shifted)
    labels = jnp.searchsorted(jnp.cumsum(lengths), jnp.arange(rows * top), side="right").astype(jnp.int32)
    listing = labels.reshape(top, rows).T
    listing = listing[jax.random.permutation(jax.random.fold_in(own, 1), rows)]
    offset_by = jax.random.randint(jax.random.fold_in(own, 2), (rows, 1), 0, top)
    return jnp.take_along_axis(listing, (jnp.arange(top)[None, :] + offset_by) % top, axis=1)


def shares(number_of, total, most, skew, full):
    weights = [(1 << 20) // math.isqrt(standing ** skew) + 1 for standing in range(1, number_of + 1)]
    largest = most if full else min(most, max(-(-total // number_of), total * weights[0] // sum(weights)))
    least = 1 if total - largest >= number_of - 1 else 0
    given, spare = [largest] + [least] * (number_of - 1), total - largest - least * (number_of - 1)
    while spare > 0:
        candidates = [i for i in range(1, number_of) if given[i] < largest] or [i for i in range(1, number_of) if given[i] < most]
        whole, left = sum([weights[i] for i in candidates]), spare
        for i in candidates:
            extra = min(most - given[i], max(1, left * weights[i] // whole), spare)
            given[i] = given[i] + extra
            spare = spare - extra
    return np.array(given)


def noise(own_key, shape, scale, most, cuts=(), held_as=jnp.bfloat16):
    result = scale * jax.random.normal(own_key, shape, jnp.float32)
    if cuts:
        result = result * steps_of(own_key, shape, cuts, -0.22, 0.18)
    return jnp.clip(result, -most, most).astype(held_as)


def noise_with(own_key, shape, spread, reach, cuts, heavy, kind=jnp.bfloat16):
    drawn = spread * jax.random.normal(own_key, shape, jnp.float32)
    if cuts:
        drawn = drawn * steps_of(own_key, shape, cuts, -0.22, 0.18)
    return jnp.clip(spiked(drawn, jax.random.fold_in(own_key, 3), *heavy), -reach, reach).astype(kind)


def setup_inputs(seed: int = 0) -> dict:
    streams_of = jax.random.split(jax.random.key(seed), 15)
    hidden_state = draw_hidden_state(jax.random.fold_in(streams_of[14], 71), 0)
    norm_gain = jnp.clip(1.0 + 0.18 * jax.random.normal(streams_of[1], (D,), jnp.float32), 0.1, 1.9)
    route_ids_keys = jax.random.split(jax.random.fold_in(streams_of[2], 1), SEQUENCE_TOKENS // TOK_DEV)
    route_ids_turns = jax.random.permutation(jax.random.fold_in(streams_of[2], 3), SEQUENCE_TOKENS // TOK_DEV)
    route_ids = jax.vmap(lambda own, number: deal_out(jax.random.fold_in(streams_of[2], 2), own, number, TOK_DEV, EXPERTS, 2, CAP, 1))(route_ids_keys, route_ids_turns).reshape((SEQUENCE_TOKENS, 2))
    route_logits = noise(streams_of[3], (SEQUENCE_TOKENS, 2), 1.0, 6.0, ((0, 8),), jnp.float32)
    cotangent = noise_with(streams_of[4], (SEQUENCE_TOKENS, D), 1.0, 6.0, ((0, 8),), (0, 1, 8, 2.0))
    w_gate = noise(streams_of[5], (EXPERTS, D, FFE), D ** -0.5, 0.125, ((0, 8), (2, 4)))
    w_up = noise(streams_of[6], (EXPERTS, D, FFE), D ** -0.5, 0.125, ((0, 8), (2, 4)))
    w_down = noise(streams_of[7], (EXPERTS, FFE, D), FFE ** -0.5, 0.15625, ((0, 8), (1, 4)))
    w_out = noise(streams_of[8], (D, HV), HV ** -0.5, 0.1875, ((1, 4),))
    query_rows = noise(streams_of[9], (SEQUENCE_TOKENS, HK), 1.0, 6.0, ((0, 8), (1, 4)))
    key_rows = noise(streams_of[10], (SEQUENCE_TOKENS, HK), 1.0, 6.0, ((0, 8), (1, 4)))
    value_rows = noise(streams_of[11], (SEQUENCE_TOKENS, HV), 1.0, 6.0, ((0, 8), (1, 4)))
    log_decay = draw_log_decay(jax.random.fold_in(streams_of[14], 71), 0)
    head_gain = jnp.clip(1.0 + 0.18 * jax.random.normal(streams_of[13], (HV,), jnp.float32), 0.1, 1.9)
    return {"hidden_state": hidden_state, "norm_gain": norm_gain, "route_ids": route_ids, "route_logits": route_logits, "cotangent": cotangent, "w_gate": w_gate, "w_up": w_up, "w_down": w_down, "w_out": w_out, "query_rows": query_rows, "key_rows": key_rows, "value_rows": value_rows, "log_decay": log_decay, "head_gain": head_gain}


exact_numeric_mode = lax.Precision.HIGHEST
eps_value = 1e-06

def blocks_of(array, width):
    return array.reshape((array.shape[0] // BLOCK, BLOCK, array.shape[1] // width, width))

def gla_forward(query_f, key_f, value_f, log_f):
    causal = jnp.arange(BLOCK)[:, None] >= jnp.arange(BLOCK)[None, :]

    def advance(carried_state, inputs):
        query_block, key_block, value_block, log_b = inputs
        cumulative_decay = jnp.cumsum(log_b, axis=0)
        decay_mid = cumulative_decay[BLOCK // 2]
        final_decay = cumulative_decay[BLOCK - 1]
        scores = jnp.einsum('thk,shk->hts', query_block * jnp.exp(cumulative_decay - decay_mid), key_block * jnp.exp(decay_mid - cumulative_decay), precision=exact_numeric_mode)
        scores = jnp.where(causal[None], scores, 0.0)
        result_output = jnp.einsum('hts,shv->thv', scores, value_block, precision=exact_numeric_mode)
        result_output = result_output + jnp.einsum('jml,mld->jmd', query_block * jnp.exp(cumulative_decay), carried_state, precision=exact_numeric_mode)
        updated_state = jnp.exp(final_decay)[:, :, None] * carried_state + jnp.einsum('yiu,yig->iug', key_block * jnp.exp(final_decay - cumulative_decay), value_block, precision=exact_numeric_mode)
        return (updated_state, result_output)
    zero_state = jnp.zeros((HEADS, KEY_DIM, VAL_DIM), jnp.float32)
    final_state, outputs = lax.scan(advance, zero_state, (blocks_of(query_f, KEY_DIM), blocks_of(key_f, KEY_DIM), blocks_of(value_f, VAL_DIM), blocks_of(log_f, KEY_DIM)))
    return outputs.reshape(SEQUENCE_TOKENS, HEADS, VAL_DIM)

def slot_numbers(ids):
    flat_ids = ids.reshape(-1)
    one_hot = (flat_ids[:, None] == jnp.arange(EXPERTS, dtype=jnp.int32)[None, :]).astype(jnp.int32)
    slot_rank = lax.optimization_barrier(jnp.sum((jnp.cumsum(one_hot, axis=0) - 1) * one_hot, axis=1))
    return (flat_ids * CAP + slot_rank).astype(jnp.int32)

def slot_sources(slots):
    row_total = slots.shape[0]
    return jnp.full((EXPERTS * CAP,), row_total, jnp.int32).at[slots].set(jnp.arange(row_total, dtype=jnp.int32))

def reference(hidden_state, norm_gain, route_ids, route_logits, cotangent, w_gate, w_up, w_down, w_out, query_rows, key_rows, value_rows, log_decay, head_gain):
    gain_heads = head_gain.reshape(HEADS, VAL_DIM)

    def mixer_fwd(query_f, key_f, value_f, log_f):
        head_out = gla_forward(query_f, key_f, value_f, log_f)
        inv_rms = lax.rsqrt(lax.optimization_barrier(jnp.mean(head_out * head_out, axis=-1, keepdims=True)) + eps_value)
        return (head_out * inv_rms * gain_heads).reshape(SEQUENCE_TOKENS, HEADS * VAL_DIM)
    mixed_f, pullback = jax.vjp(mixer_fwd, query_rows.astype(jnp.float32), key_rows.astype(jnp.float32), value_rows.astype(jnp.float32), log_decay)
    mixed_out = mixed_f.astype(jnp.bfloat16)
    state_f = hidden_state.astype(jnp.float32)
    row_scale = lax.rsqrt(lax.optimization_barrier(jnp.mean(state_f * state_f, axis=-1, keepdims=True)) + eps_value)
    unit_rows = state_f * row_scale
    normed_in = (unit_rows * norm_gain).astype(jnp.bfloat16)
    route_weight = jax.nn.softmax(route_logits, axis=-1)
    cot_f = cotangent.astype(jnp.float32)
    slot_grads = (route_weight[:, :, None] * cot_f[:, None, :]).astype(jnp.bfloat16).reshape(2 * SEQUENCE_TOKENS, D)
    slots = jax.vmap(slot_numbers)(route_ids.reshape(N_SP, TOK_DEV, 2))
    sources = jax.vmap(slot_sources)(slots)
    offsets = (jnp.arange(N_SP, dtype=jnp.int32) * (2 * TOK_DEV))[:, None]
    global_src = jnp.where(sources < 2 * TOK_DEV, sources + offsets, 2 * SEQUENCE_TOKENS).astype(jnp.int32)
    by_expert = global_src.reshape(N_SP, EXPERTS, CAP).transpose(1, 0, 2).reshape(EXPERTS, N_SP * CAP)
    padded_in = jnp.concatenate([normed_in, jnp.zeros((1, D), jnp.bfloat16)], axis=0)
    padded_grad = jnp.concatenate([slot_grads, jnp.zeros((1, D), jnp.bfloat16)], axis=0)
    part_width = FFE // N_TP

    def one_expert(returned, inputs):
        rows_src, gate_w, up_w, down_w = inputs
        rows_in = padded_in[jnp.where(rows_src < 2 * SEQUENCE_TOKENS, rows_src // 2, SEQUENCE_TOKENS).astype(jnp.int32)]
        rows_grad = padded_grad[rows_src]
        gate_pre = jnp.dot(rows_in, gate_w, preferred_element_type=jnp.float32)
        up_pre = jnp.dot(rows_in, up_w, preferred_element_type=jnp.float32)
        gate_sig = jax.nn.sigmoid(gate_pre)
        silu_gate = gate_pre * gate_sig
        hidden_units = (silu_gate * up_pre).astype(jnp.bfloat16)
        grad_down = jnp.dot(hidden_units.T, rows_grad, preferred_element_type=jnp.float32)
        grad_hidden = jnp.dot(rows_grad, down_w.T, preferred_element_type=jnp.float32)
        grad_gate_pre = (grad_hidden * up_pre * gate_sig * (1.0 + gate_pre * (1.0 - gate_sig))).astype(jnp.bfloat16)
        grad_up_pre = (grad_hidden * silu_gate).astype(jnp.bfloat16)
        grad_gate = jnp.dot(rows_in.T, grad_gate_pre, preferred_element_type=jnp.float32)
        grad_up = jnp.dot(rows_in.T, grad_up_pre, preferred_element_type=jnp.float32)
        summed_rows = jnp.zeros((N_SP * CAP, D), jnp.float32)
        for group_index in range(N_TP):
            lower = group_index * part_width
            upper = lower + part_width
            partial_piece = jnp.dot(grad_gate_pre[:, lower:upper], gate_w[:, lower:upper].T, preferred_element_type=jnp.float32)
            partial_piece = partial_piece + jnp.dot(grad_up_pre[:, lower:upper], up_w[:, lower:upper].T, preferred_element_type=jnp.float32)
            rounded_piece = lax.optimization_barrier(partial_piece.astype(jnp.bfloat16))
            summed_rows = summed_rows + rounded_piece.astype(jnp.float32)
        returned = returned.at[rows_src].set(summed_rows.astype(jnp.bfloat16), mode='drop')
        return (returned, (grad_gate.astype(jnp.bfloat16), grad_up.astype(jnp.bfloat16), grad_down.astype(jnp.bfloat16)))
    slot_back, expert_grads = lax.scan(one_expert, jnp.zeros((2 * SEQUENCE_TOKENS, D), jnp.bfloat16), (by_expert, w_gate, w_up, w_down))
    grad_normed = lax.optimization_barrier(jnp.sum(slot_back.astype(jnp.float32).reshape(SEQUENCE_TOKENS, 2, D), axis=1))
    grad_unit = grad_normed * norm_gain
    grad_state = row_scale * (grad_unit - unit_rows * lax.optimization_barrier(jnp.mean(grad_unit * unit_rows, axis=-1, keepdims=True)))
    grad_mixed = (cot_f + grad_state).astype(jnp.bfloat16)
    grad_out_w = jnp.dot(grad_mixed.T, mixed_out, preferred_element_type=jnp.float32)
    grad_mix = jnp.dot(grad_mixed, w_out, preferred_element_type=jnp.float32).astype(jnp.bfloat16)
    grad_mix = lax.optimization_barrier(grad_mix).astype(jnp.float32)
    grad_query, grad_key, grad_value, grad_log = pullback(grad_mix)
    return (expert_grads[0], expert_grads[1], expert_grads[2], grad_out_w, grad_query.astype(jnp.bfloat16), grad_key.astype(jnp.bfloat16), grad_value.astype(jnp.bfloat16), grad_log)
```

```python
import functools
import jax
import jax.numpy as jnp
from jax import lax
from jax.experimental import pallas as pl
from jax.experimental.pallas import tpu as pltpu
from jax.sharding import PartitionSpec as P

KEY_DIM = 64
VAL_DIM = 128
BLOCK = 64
MESH = pl.DeviceIdType.MESH


exact_numeric_mode = lax.Precision.HIGHEST
eps_value = 1e-06


def remote(src, dst, send, recv, sp, tp):
    return pltpu.make_async_remote_copy(
        src_ref=src, dst_ref=dst, send_sem=send, recv_sem=recv, device_id=(sp, tp), device_id_type=MESH
    )


def each(start, stop, step):
    lax.fori_loop(start, stop, lambda k, _: (step(k), 0)[1], 0)


def greet(n, me, tp, others):
    barrier = pltpu.get_barrier_semaphore()

    def hello(k):
        pl.semaphore_signal(
            barrier, inc=1, device_id=(lax.rem(me + k, n), tp), device_id_type=MESH
        )

    if n > 1:
        each(1, n, hello)
    for sp, other in others:
        pl.semaphore_signal(barrier, inc=1, device_id=(sp, other), device_id_type=MESH)
    pl.semaphore_wait(barrier, n - 1 + len(others))


class Carry:
    def __init__(self, n, me, tp, reverse, first, held, sent, scan, send_sem, recv_sem):
        self.n, self.me, self.tp, self.reverse = n, me, tp, reverse
        self.first, self.held, self.sent, self.scan = first, held, sent, scan
        self.send_sem, self.recv_sem = send_sem, recv_sem
        self.rows = first.shape[0] - 8
        self.scan[...] = jnp.zeros_like(self.scan)

    def parts(self, step):
        d = 1 << step
        n, me = self.n, self.me
        if self.reverse:
            to, has_to, has_from = lax.rem(me - d + n, n), me >= d, me + d < n
        else:
            to, has_to, has_from = lax.rem(me + d, n), me + d < n, me >= d
        src = self.first if step == 0 else self.sent.at[step - 1]
        copy = remote(
            src, self.held.at[step], self.send_sem.at[step], self.recv_sem.at[step], to, self.tp
        )
        return copy, has_to, has_from

    def send(self, step):
        copy, has_to, _ = self.parts(step)
        pl.when(has_to)(lambda: copy.start())

    def receive(self, step, last):
        copy, _, has_from = self.parts(step)
        rows = self.rows
        now = self.first if step == 0 else self.sent.at[step - 1]

        @pl.when(has_from)
        def _():
            copy.wait_recv()

        if not last:

            @pl.when(has_from)
            def _():
                other = self.held[step]
                mine = now[...]
                self.sent[step] = mine[rows : rows + 1] * other
                self.sent[step, :rows] += mine[:rows]

            @pl.when(jnp.logical_not(has_from))
            def _():
                self.sent[step] = now[...]

        @pl.when(has_from)
        def _():
            other = self.held[step]
            if step == 0:
                self.scan[...] = other
            else:
                mine = self.scan[...]
                self.scan[...] = mine[rows : rows + 1] * other
                self.scan[:rows, :] += mine[:rows]

    def finish(self, steps):
        for step in range(steps):
            copy, has_to, _ = self.parts(step)
            pl.when(has_to)(lambda copy=copy: copy.wait_send())


def steps_of(n):
    return max(1, (n - 1).bit_length())


def carry_scratch(n, shape):
    steps = steps_of(n)
    return [
        pltpu.VMEM((steps,) + shape, jnp.float32),
        pltpu.VMEM((steps,) + shape, jnp.float32),
        pltpu.SemaphoreType.DMA((steps,)),
        pltpu.SemaphoreType.DMA((steps,)),
    ]


def tp_pair(tp):
    return tp + 1 - 2 * lax.rem(tp, 2), lax.rem(tp + 2, 4)


def dispatch_kernel(
    n,
    a_ref,
    b_ref,
    state_ref,
    a_out,
    b_out,
    scan_out,
    held,
    sent,
    carry_send,
    carry_recv,
    local_sem,
    send_sem,
    recv_sem,
    pair_send,
    pair_recv,
    twin_send,
    twin_recv,
):
    me, tp = lax.axis_index("sp"), lax.axis_index("tp")
    pair, twin = tp_pair(tp)
    width = a_ref.shape[2]
    greet(n, me, tp, [(me, pair), (me, twin)])
    steps = steps_of(n)
    carry = Carry(n, me, tp, False, state_ref, held, sent, scan_out, carry_send, carry_recv)
    ins, outs = (a_ref, b_ref), (a_out, b_out)

    def lanes(t):
        return pl.ds(pl.multiple_of(t * width, 128), width)

    def exchange(j, k):
        to = lax.rem(me + k, n)
        return remote(
            ins[j].at[to],
            outs[j].at[me, :, lanes(tp)],
            send_sem.at[j, k],
            recv_sem.at[j, k],
            to,
            tp,
        )

    def own(j):
        return pltpu.make_async_copy(
            ins[j].at[me], outs[j].at[me, :, lanes(tp)], local_sem.at[j]
        )

    def forward(j, k, kind):
        block = lax.rem(me - k + n, n)
        if kind == 0:
            piece = outs[j].at[block, :, lanes(tp)]
            return remote(
                piece, piece, twin_send.at[j, k], twin_recv.at[j, k], me, twin
            )
        piece = outs[j].at[block, :, lanes(tp if kind == 1 else twin)]
        return remote(
            piece, piece, pair_send.at[j, kind - 1, k], pair_recv.at[j, kind - 1, k], me, pair
        )

    def spread(j, k):
        exchange(j, k).wait_recv()
        forward(j, k, 0).start()
        forward(j, k, 1).start()

    def begin(j):
        own(j).start()
        each(1, n, lambda k: exchange(j, k).start())
        own(j).wait()
        forward(j, 0, 0).start()
        forward(j, 0, 1).start()

    def twin_done(j, k):
        block = lax.rem(me - k + n, n)
        forward(j, k, 0).wait_recv()
        forward(j, k, 2).start()

    half = n // 2
    carry.send(0)
    begin(0)
    carry.receive(0, steps == 1)
    if steps > 1:
        carry.send(1)
    each(1, half, lambda k: spread(0, k))
    begin(1)
    each(half, n, lambda k: spread(0, k))
    for step in range(1, steps):
        carry.receive(step, step == steps - 1)
        if step + 1 < steps:
            carry.send(step + 1)
    each(1, half, lambda k: spread(1, k))
    each(0, n, lambda k: twin_done(0, k))
    each(half, n, lambda k: spread(1, k))
    each(0, n, lambda k: twin_done(1, k))
    carry.finish(steps)
    for j in range(2):
        each(1, n, lambda k: exchange(j, k).wait_send())

        def finish(k):
            forward(j, k, 0).wait_send()
            for kind in (1, 2):
                forward(j, k, kind).wait()

        each(0, n, finish)


def vmem(count):
    return [pl.BlockSpec(memory_space=pltpu.VMEM)] * count


def dispatch(n, part_in, part_grad, packed):
    count, cap, width = part_in.shape
    full = jax.ShapeDtypeStruct((count, cap, 4 * width), part_in.dtype)
    dma = pltpu.SemaphoreType.DMA
    return pl.pallas_call(
        functools.partial(dispatch_kernel, n),
        out_shape=[full, full, jax.ShapeDtypeStruct(packed.shape, jnp.float32)],
        in_specs=vmem(3),
        out_specs=vmem(3),
        scratch_shapes=carry_scratch(n, packed.shape)
        + [
            dma((2,)),
            dma((2, n)),
            dma((2, n)),
            dma((2, 2, n)),
            dma((2, 2, n)),
            dma((2, n)),
            dma((2, n)),
        ],
        compiler_params=pltpu.CompilerParams(
            collective_id=0, has_side_effects=True, vmem_limit_bytes=40 << 20
        ),
        name="dispatch",
    )(part_in, part_grad, packed)


def return_kernel(
    n,
    part_ref,
    mix_ref,
    back_out,
    mix_out,
    near,
    far_sum,
    far,
    total,
    local_sem,
    near_send,
    near_recv,
    far_send,
    far_recv,
    send_sem,
    recv_sem,
    mix_send,
    mix_recv,
):
    me, tp = lax.axis_index("sp"), lax.axis_index("tp")
    pair, twin = tp_pair(tp)
    pair_twin = lax.rem(pair + 2, 4)
    width = back_out.shape[2]
    greet(n, me, tp, [(me, pair), (me, twin)])

    def lanes(t):
        return pl.ds(pl.multiple_of(t * width, 128), width)

    def to_pair(kind, k):
        block = lax.rem(me + k, n)
        return remote(
            part_ref.at[block, :, lanes(pair if kind == 0 else pair_twin)],
            near.at[kind, block],
            near_send.at[kind, k],
            near_recv.at[kind, k],
            me,
            pair,
        )

    def to_twin(k):
        block = lax.rem(me + k, n)
        return remote(far_sum.at[block], far.at[block], far_send.at[k], far_recv.at[k], me, twin)

    def to_owner(k):
        block = lax.rem(me + k, n)
        return remote(total.at[block], back_out.at[me], send_sem.at[k], recv_sem.at[k], block, tp)

    def mixed(k):
        to = lax.rem(me + k, n)
        return remote(mix_ref, mix_out.at[me], mix_send.at[k], mix_recv.at[k], to, tp)

    each(1, n + 1, lambda k: to_pair(1, lax.rem(k, n)).start())
    each(1, n + 1, lambda k: to_pair(0, lax.rem(k, n)).start())
    each(1, n, lambda k: mixed(k).start())
    own_mix = pltpu.make_async_copy(mix_ref, mix_out.at[me], local_sem.at[0])
    own_mix.start()

    def reduce_pair(i):
        k = lax.rem(i, n)
        block = lax.rem(me + k, n)
        to_pair(1, k).wait_recv()
        mine = part_ref[block, :, lanes(twin)].astype(jnp.float32)
        far_sum[block] = (mine + near[1, block].astype(jnp.float32)).astype(jnp.bfloat16)
        pl.when(i > 1)(lambda: to_twin(i - 1).start())

    each(1, n + 1, reduce_pair)
    to_twin(0).start()

    def reduce_all(i):
        k = lax.rem(i, n)
        block = lax.rem(me + k, n)
        to_pair(0, k).wait_recv()
        to_twin(k).wait_recv()
        mine = part_ref[block, :, lanes(tp)].astype(jnp.float32)
        mine = mine + near[0, block].astype(jnp.float32) + far[block].astype(jnp.float32)
        total[block] = mine.astype(jnp.bfloat16)
        pl.when(i > 1)(lambda: to_owner(i - 1).start())

    each(1, n + 1, reduce_all)
    back_out[me] = total[me]
    own_mix.wait()

    def finish(k):
        for kind in (0, 1):
            to_pair(kind, k).wait_send()
        to_twin(k).wait_send()

    each(0, n, finish)

    def finish_far(k):
        to_owner(k).wait()
        mixed(k).wait()

    each(1, n, finish_far)


def give_back(n, partial_rows, mixed_out):
    count, cap, model_width = partial_rows.shape
    width = model_width // 4
    dma = pltpu.SemaphoreType.DMA
    block = (count, cap, width)
    return pl.pallas_call(
        functools.partial(return_kernel, n),
        out_shape=[
            jax.ShapeDtypeStruct(block, jnp.bfloat16),
            jax.ShapeDtypeStruct((n,) + mixed_out.shape, jnp.bfloat16),
        ],
        in_specs=vmem(2),
        out_specs=vmem(2),
        scratch_shapes=[
            pltpu.VMEM((2,) + block, jnp.bfloat16),
            pltpu.VMEM(block, jnp.bfloat16),
            pltpu.VMEM(block, jnp.bfloat16),
            pltpu.VMEM(block, jnp.bfloat16),
            dma((1,)),
            dma((2, n)),
            dma((2, n)),
            dma((n,)),
            dma((n,)),
            dma((n,)),
            dma((n,)),
            dma((n,)),
            dma((n,)),
        ],
        compiler_params=pltpu.CompilerParams(
            collective_id=1, has_side_effects=True, vmem_limit_bytes=40 << 20
        ),
        name="give_back",
    )(partial_rows, mixed_out)


def features_kernel(x_ref, out_ref, local_sem, send_sem, recv_sem):
    me, tp = lax.axis_index("sp"), lax.axis_index("tp")
    pair, twin = tp_pair(tp)
    greet(1, me, tp, [(me, pair), (me, twin)])
    own = pltpu.make_async_copy(x_ref, out_ref.at[tp], local_sem.at[0])
    own.start()
    copies = [
        remote(x_ref, out_ref.at[tp], send_sem.at[0], recv_sem.at[0], me, twin),
        remote(x_ref, out_ref.at[tp], send_sem.at[1], recv_sem.at[1], me, pair),
        remote(out_ref.at[twin], out_ref.at[twin], send_sem.at[2], recv_sem.at[2], me, pair),
    ]
    copies[0].start()
    copies[1].start()
    copies[0].wait_recv()
    copies[2].start()
    copies[1].wait()
    copies[2].wait()
    copies[0].wait_send()
    own.wait()


def all_features(x):
    dma = pltpu.SemaphoreType.DMA
    return pl.pallas_call(
        features_kernel,
        out_shape=jax.ShapeDtypeStruct((4,) + x.shape, x.dtype),
        in_specs=vmem(1),
        out_specs=pl.BlockSpec(memory_space=pltpu.VMEM),
        scratch_shapes=[dma((1,)), dma((3,)), dma((3,))],
        compiler_params=pltpu.CompilerParams(collective_id=2, has_side_effects=True),
        name="all_features",
    )(x)


def last_kernel(
    n, rows_ref, state_ref, rows_out, scan_out, held, sent, carry_send, carry_recv, local_sem, send_sem, recv_sem
):
    me, tp = lax.axis_index("sp"), lax.axis_index("tp")
    greet(n, me, tp, [])
    steps = steps_of(n)
    carry = Carry(n, me, tp, True, state_ref, held, sent, scan_out, carry_send, carry_recv)

    def exchange(k):
        to = lax.rem(me + k, n)
        return remote(rows_ref.at[to], rows_out.at[me], send_sem.at[k], recv_sem.at[k], to, tp)

    own = pltpu.make_async_copy(rows_ref.at[me], rows_out.at[me], local_sem.at[0])
    carry.send(0)
    own.start()
    cuts = [1 + (n - 1) * i // steps for i in range(steps + 1)]
    for step in range(steps):
        each(cuts[step], cuts[step + 1], lambda k: exchange(k).start())
        carry.receive(step, step == steps - 1)
        if step + 1 < steps:
            carry.send(step + 1)
    carry.finish(steps)
    own.wait()
    each(1, n, lambda k: exchange(k).wait())


def last_exchange(n, rows, packed):
    dma = pltpu.SemaphoreType.DMA
    return pl.pallas_call(
        functools.partial(last_kernel, n),
        out_shape=[
            jax.ShapeDtypeStruct(rows.shape, rows.dtype),
            jax.ShapeDtypeStruct(packed.shape, jnp.float32),
        ],
        in_specs=vmem(2),
        out_specs=vmem(2),
        scratch_shapes=carry_scratch(n, packed.shape) + [dma((1,)), dma((n,)), dma((n,))],
        compiler_params=pltpu.CompilerParams(
            collective_id=3, has_side_effects=True, vmem_limit_bytes=40 << 20
        ),
        name="last_exchange",
    )(rows, packed)


def pack_state(state, decay):
    heads, keys, values = state.shape
    rows = state.transpose(2, 0, 1).reshape(values, heads * keys)
    return jnp.concatenate([rows, jnp.broadcast_to(decay.reshape(1, -1), (8, heads * keys))], axis=0)


def unpack_state(packed, heads):
    rows = packed[:-8]
    return rows.reshape(rows.shape[0], heads, -1).transpose(1, 2, 0)


def carry_blocks(carried_state, inputs):
    decay_now, term_now = inputs
    return (decay_now[:, :, None] * carried_state + term_now, carried_state)


def block_scan(decays, terms, state, reverse):
    count = decays.shape[0]
    starts = [None] * count
    for i in reversed(range(count)) if reverse else range(count):
        state, starts[i] = carry_blocks(state, (decays[i], terms[i]))
    return state, jnp.stack(starts)


def body(
    hidden_state,
    norm_gain,
    route_ids,
    route_logits,
    cotangent,
    w_gate,
    w_up,
    w_down,
    w_out,
    query_rows,
    key_rows,
    value_rows,
    log_decay,
    head_gain,
):
    tok_count, model_width = hidden_state.shape
    head_count = head_gain.shape[0] // VAL_DIM
    block_count = tok_count // BLOCK
    shape_key = (block_count, BLOCK, head_count, KEY_DIM)
    shape_value = (block_count, BLOCK, head_count, VAL_DIM)
    query_f = query_rows.astype(jnp.float32).reshape(shape_key)
    key_f = key_rows.astype(jnp.float32).reshape(shape_key)
    value_f = value_rows.astype(jnp.float32).reshape(shape_value)
    cumulative_decay = jnp.cumsum(log_decay.reshape(shape_key), axis=1)
    decay_mid = cumulative_decay[:, BLOCK // 2 : BLOCK // 2 + 1]
    final_decay = cumulative_decay[:, BLOCK - 1 : BLOCK]
    query_in = query_f * jnp.exp(cumulative_decay - decay_mid)
    key_in = key_f * jnp.exp(decay_mid - cumulative_decay)
    key_end = key_f * jnp.exp(final_decay - cumulative_decay)
    query_start = query_f * jnp.exp(cumulative_decay)
    causal = (jnp.arange(BLOCK)[:, None] >= jnp.arange(BLOCK)[None, :])[None, None]
    last_logs = final_decay[:, 0]
    through = jnp.cumsum(last_logs, axis=0)
    total_log = through[-1]
    total_decay = jnp.exp(total_log)
    block_decay = jnp.exp(last_logs)
    block_kv = jnp.einsum("bshk,bshv->bhkv", key_end, value_f, precision=exact_numeric_mode)
    zero_state = jnp.zeros((head_count, KEY_DIM, VAL_DIM), jnp.float32)
    ones_decay = jnp.ones_like(total_log)
    local_end, local_start = block_scan(block_decay, block_kv, zero_state, False)
    sp_count = lax.axis_size("sp")
    state_f = hidden_state.astype(jnp.float32)
    row_scale = lax.rsqrt(jnp.mean(state_f * state_f, axis=-1, keepdims=True) + eps_value)
    part_width = model_width // lax.axis_size("tp")
    feature_start = lax.axis_index("tp") * part_width
    hidden_part = lax.dynamic_slice_in_dim(hidden_state, feature_start, part_width, 1)
    gain_part = lax.dynamic_slice_in_dim(norm_gain, feature_start, part_width, 0)
    cot_part = lax.dynamic_slice_in_dim(cotangent, feature_start, part_width, 1)
    normed_part = (hidden_part.astype(jnp.float32) * row_scale * gain_part).astype(jnp.bfloat16)
    route_weight = jax.nn.softmax(route_logits, axis=-1)
    expert_count = sp_count
    capacity = 4 * tok_count // expert_count
    named = route_ids[:, :, None] == jnp.arange(expert_count, dtype=jnp.int32)[None, None, :]
    names = jnp.any(named, axis=1)
    weight_of = jnp.sum(jnp.where(named, route_weight[:, :, None], 0.0), axis=1)
    before = (jnp.arange(tok_count)[:, None] > jnp.arange(tok_count)[None, :]).astype(jnp.bfloat16)
    rank = jnp.dot(before, names.astype(jnp.bfloat16), preferred_element_type=jnp.float32)
    place = jnp.where(names, rank, -1.0).T
    filled = place[:, None, :] == jnp.arange(capacity, dtype=jnp.float32)[None, :, None]
    slot_weight = jnp.sum(jnp.where(filled, weight_of.T[:, None, :], 0.0), axis=2)
    pick = filled.astype(jnp.bfloat16).reshape(expert_count * capacity, tok_count)
    send_in = jnp.dot(pick, normed_part, preferred_element_type=jnp.float32).astype(jnp.bfloat16)
    send_grad = jnp.dot(pick, cot_part, preferred_element_type=jnp.float32)
    send_grad = (send_grad * slot_weight.reshape(-1, 1)).astype(jnp.bfloat16)
    got_in, got_grad, scanned = dispatch(
        sp_count,
        send_in.reshape(expert_count, capacity, part_width),
        send_grad.reshape(expert_count, capacity, part_width),
        pack_state(local_end, total_decay),
    )
    state_in = unpack_state(scanned, head_count)
    block_states = local_start + jnp.exp(through - last_logs)[:, :, :, None] * state_in
    end_state = total_decay[:, :, None] * state_in + local_end
    scores = jnp.where(
        causal, jnp.einsum("bthk,bshk->bhts", query_in, key_in, precision=exact_numeric_mode), 0.0
    )
    head_out = jnp.einsum("bhts,bshv->bthv", scores, value_f, precision=exact_numeric_mode)
    head_out = head_out + jnp.einsum(
        "bthk,bhkv->bthv", query_start, block_states, precision=exact_numeric_mode
    )
    inv_rms = lax.rsqrt(jnp.mean(head_out * head_out, axis=-1, keepdims=True) + eps_value)
    normed = head_out * inv_rms
    gain_heads = head_gain.reshape(head_count, VAL_DIM)
    mixed_out = (normed * gain_heads).reshape(tok_count, head_count * VAL_DIM).astype(jnp.bfloat16)
    unit_rows = state_f * row_scale
    cot_f = cotangent.astype(jnp.float32)
    rows_in = got_in.reshape(-1, model_width)
    rows_grad = got_grad.reshape(-1, model_width)
    gate_w = w_gate[0]
    up_w = w_up[0]
    down_w = w_down[0]
    gate_pre = jnp.dot(rows_in, gate_w, preferred_element_type=jnp.float32)
    up_pre = jnp.dot(rows_in, up_w, preferred_element_type=jnp.float32)
    gate_sig = jax.nn.sigmoid(gate_pre)
    silu_gate = gate_pre * gate_sig
    hidden_units = (silu_gate * up_pre).astype(jnp.bfloat16)
    grad_down = jnp.einsum("rf,rd->fd", hidden_units, rows_grad, preferred_element_type=jnp.float32)
    grad_hidden = jnp.einsum("rd,fd->rf", rows_grad, down_w, preferred_element_type=jnp.float32)
    grad_gate_pre = (grad_hidden * up_pre * gate_sig * (1.0 + gate_pre * (1.0 - gate_sig))).astype(
        jnp.bfloat16
    )
    grad_up_pre = (grad_hidden * silu_gate).astype(jnp.bfloat16)
    grad_gate_w = jnp.einsum(
        "rd,rf->df", rows_in, grad_gate_pre, preferred_element_type=jnp.float32
    )
    grad_up_w = jnp.einsum("rd,rf->df", rows_in, grad_up_pre, preferred_element_type=jnp.float32)
    partial_rows = jnp.einsum(
        "rf,df->rd", grad_gate_pre, gate_w, preferred_element_type=jnp.float32
    )
    partial_rows = partial_rows + jnp.einsum(
        "rf,df->rd", grad_up_pre, up_w, preferred_element_type=jnp.float32
    )
    partial_rows = partial_rows.reshape(expert_count, capacity, model_width)
    returned, mixed_all = give_back(sp_count, partial_rows.astype(jnp.bfloat16), mixed_out)
    summed = lax.dot_general(
        pick,
        returned.reshape(-1, part_width),
        (((0,), (0,)), ((), ())),
        preferred_element_type=jnp.float32,
    )
    grad_normed = all_features(summed.astype(jnp.bfloat16)).astype(jnp.float32)
    grad_normed = grad_normed.transpose(1, 0, 2).reshape(tok_count, model_width)
    grad_unit = grad_normed * norm_gain
    grad_state = row_scale * (
        grad_unit - unit_rows * jnp.mean(grad_unit * unit_rows, axis=-1, keepdims=True)
    )
    grad_mixed = (cot_f + grad_state).astype(jnp.bfloat16)
    grad_mix = jnp.dot(grad_mixed, w_out, preferred_element_type=jnp.float32).astype(jnp.bfloat16)
    grad_mix = lax.optimization_barrier(grad_mix).astype(jnp.float32).reshape(shape_value)
    grad_scaled = grad_mix * gain_heads
    grad_out = inv_rms * (
        grad_scaled - normed * jnp.mean(grad_scaled * normed, axis=-1, keepdims=True)
    )
    block_adj = jnp.einsum("bthk,bthv->bhkv", query_start, grad_out, precision=exact_numeric_mode)
    local_adj, later_adj = block_scan(block_decay, block_adj, zero_state, True)
    mixed_parts = grad_mixed.reshape(tok_count, sp_count, -1).transpose(1, 0, 2)
    got_mixed, behind = last_exchange(sp_count, mixed_parts, pack_state(local_adj, total_decay))
    grad_out_w = jnp.einsum("ntd,nth->dh", got_mixed, mixed_all, preferred_element_type=jnp.float32)
    adj_end = unpack_state(behind, head_count)
    block_adj_end = later_adj + jnp.exp(total_log - through)[:, :, :, None] * adj_end
    grad_dots = jnp.where(
        causal, jnp.einsum("bthv,bshv->bhts", grad_out, value_f, precision=exact_numeric_mode), 0.0
    )
    grad_query = jnp.exp(cumulative_decay - decay_mid) * jnp.einsum(
        "bhts,bshk->bthk", grad_dots, key_in, precision=exact_numeric_mode
    )
    grad_query = grad_query + jnp.exp(cumulative_decay) * jnp.einsum(
        "bthv,bhkv->bthk", grad_out, block_states, precision=exact_numeric_mode
    )
    grad_key = jnp.exp(decay_mid - cumulative_decay) * jnp.einsum(
        "bhts,bthk->bshk", grad_dots, query_in, precision=exact_numeric_mode
    )
    grad_key = grad_key + jnp.exp(final_decay - cumulative_decay) * jnp.einsum(
        "bhkv,bshv->bshk", block_adj_end, value_f, precision=exact_numeric_mode
    )
    grad_value = jnp.einsum("bhts,bthv->bshv", scores, grad_out, precision=exact_numeric_mode)
    grad_value = grad_value + jnp.einsum(
        "bshk,bhkv->bshv", key_end, block_adj_end, precision=exact_numeric_mode
    )
    log_terms = (query_f * grad_query - key_f * grad_key).reshape(tok_count, head_count * KEY_DIM)
    suffix = lax.cumsum(log_terms, axis=0, reverse=True)
    tail_term = jnp.sum(adj_end * end_state, axis=-1).reshape(1, head_count * KEY_DIM)
    grad_log = suffix + tail_term
    return (
        grad_gate_w.astype(jnp.bfloat16)[None],
        grad_up_w.astype(jnp.bfloat16)[None],
        grad_down.astype(jnp.bfloat16)[None],
        grad_out_w,
        grad_query.reshape(tok_count, -1).astype(jnp.bfloat16),
        grad_key.reshape(tok_count, -1).astype(jnp.bfloat16),
        grad_value.reshape(tok_count, -1).astype(jnp.bfloat16),
        grad_log,
    )


def solution(mesh):
    in_specs = (
        P("sp", None),
        P(),
        P("sp", None),
        P("sp", None),
        P("sp", None),
        P("sp", None, "tp"),
        P("sp", None, "tp"),
        P("sp", "tp", None),
        P(None, "tp"),
        P("sp", "tp"),
        P("sp", "tp"),
        P("sp", "tp"),
        P("sp", "tp"),
        P("tp"),
    )
    out_specs = (
        P("sp", None, "tp"),
        P("sp", None, "tp"),
        P("sp", "tp", None),
        P("sp", "tp"),
        P("sp", "tp"),
        P("sp", "tp"),
        P("sp", "tp"),
        P("sp", "tp"),
    )
    return jax.shard_map(body, mesh=mesh, in_specs=in_specs, out_specs=out_specs, check_vma=False)
```

```python
import functools
import jax
import jax.numpy as jnp
from jax import lax
from jax.experimental import pallas as pl
from jax.experimental.pallas import tpu as pltpu
from jax.sharding import PartitionSpec as P

KEY_DIM = 64
VAL_DIM = 128
BLOCK = 64
MESH = pl.DeviceIdType.MESH


exact_numeric_mode = lax.Precision.HIGHEST
eps_value = 1e-06


def remote(src, dst, send, recv, sp, tp):
    return pltpu.make_async_remote_copy(
        src_ref=src, dst_ref=dst, send_sem=send, recv_sem=recv, device_id=(sp, tp), device_id_type=MESH
    )


def each(start, stop, step):
    lax.fori_loop(start, stop, lambda k, _: (step(k), 0)[1], 0)


def greet(n, me, tp, others):
    barrier = pltpu.get_barrier_semaphore()

    def hello(k):
        pl.semaphore_signal(
            barrier, inc=1, device_id=(lax.rem(me + k, n), tp), device_id_type=MESH
        )

    if n > 1:
        each(1, n, hello)
    for sp, other in others:
        pl.semaphore_signal(barrier, inc=1, device_id=(sp, other), device_id_type=MESH)
    pl.semaphore_wait(barrier, n - 1 + len(others))


class Carry:
    def __init__(self, n, me, tp, reverse, first, held, sent, scan, send_sem, recv_sem):
        self.n, self.me, self.tp, self.reverse = n, me, tp, reverse
        self.first, self.held, self.sent, self.scan = first, held, sent, scan
        self.send_sem, self.recv_sem = send_sem, recv_sem
        self.rows = first.shape[0] - 8
        self.scan[...] = jnp.zeros_like(self.scan)

    def parts(self, step):
        d = 1 << step
        n, me = self.n, self.me
        if self.reverse:
            to, has_to, has_from = lax.rem(me - d + n, n), me >= d, me + d < n
        else:
            to, has_to, has_from = lax.rem(me + d, n), me + d < n, me >= d
        src = self.first if step == 0 else self.sent.at[step - 1]
        copy = remote(
            src, self.held.at[step], self.send_sem.at[step], self.recv_sem.at[step], to, self.tp
        )
        return copy, has_to, has_from

    def send(self, step):
        copy, has_to, _ = self.parts(step)
        pl.when(has_to)(lambda: copy.start())

    def receive(self, step, last):
        copy, _, has_from = self.parts(step)
        rows = self.rows
        now = self.first if step == 0 else self.sent.at[step - 1]

        @pl.when(has_from)
        def _():
            copy.wait_recv()

        if not last:

            @pl.when(has_from)
            def _():
                other = self.held[step]
                mine = now[...]
                self.sent[step] = mine[rows : rows + 1] * other
                self.sent[step, :rows] += mine[:rows]

            @pl.when(jnp.logical_not(has_from))
            def _():
                self.sent[step] = now[...]

        @pl.when(has_from)
        def _():
            other = self.held[step]
            if step == 0:
                self.scan[...] = other
            else:
                mine = self.scan[...]
                self.scan[...] = mine[rows : rows + 1] * other
                self.scan[:rows, :] += mine[:rows]

    def finish(self, steps):
        for step in range(steps):
            copy, has_to, _ = self.parts(step)
            pl.when(has_to)(lambda copy=copy: copy.wait_send())


def steps_of(n):
    return max(1, (n - 1).bit_length())


def carry_scratch(n, shape):
    steps = steps_of(n)
    return [
        pltpu.VMEM((steps,) + shape, jnp.float32),
        pltpu.VMEM((steps,) + shape, jnp.float32),
        pltpu.SemaphoreType.DMA((steps,)),
        pltpu.SemaphoreType.DMA((steps,)),
    ]


def tp_pair(tp):
    return tp + 1 - 2 * lax.rem(tp, 2), lax.rem(tp + 2, 4)


def dispatch_kernel(
    n,
    hidden_ref,
    cot_ref,
    gain_ref,
    pick_ref,
    weight_ref,
    state_ref,
    a_out,
    b_out,
    scan_out,
    held,
    sent,
    carry_send,
    carry_recv,
    a_ref,
    b_ref,
    normed,
    local_sem,
    send_sem,
    recv_sem,
    pair_send,
    pair_recv,
    twin_send,
    twin_recv,
):
    me, tp = lax.axis_index("sp"), lax.axis_index("tp")
    pair, twin = tp_pair(tp)
    width = a_ref.shape[2]
    greet(n, me, tp, [(me, pair), (me, twin)])
    steps = steps_of(n)
    carry = Carry(n, me, tp, False, state_ref, held, sent, scan_out, carry_send, carry_recv)
    ins, outs = (a_ref, b_ref), (a_out, b_out)

    def lanes(t):
        return pl.ds(pl.multiple_of(t * width, 128), width)

    def exchange(j, k):
        to = lax.rem(me + k, n)
        return remote(
            ins[j].at[to],
            outs[j].at[me, :, lanes(tp)],
            send_sem.at[j, k],
            recv_sem.at[j, k],
            to,
            tp,
        )

    def own(j):
        return pltpu.make_async_copy(
            ins[j].at[me], outs[j].at[me, :, lanes(tp)], local_sem.at[j]
        )

    def forward(j, k, kind):
        block = lax.rem(me - k + n, n)
        if kind == 0:
            piece = outs[j].at[block, :, lanes(tp)]
            return remote(
                piece, piece, twin_send.at[j, k], twin_recv.at[j, k], me, twin
            )
        piece = outs[j].at[block, :, lanes(tp if kind == 1 else twin)]
        return remote(
            piece, piece, pair_send.at[j, kind - 1, k], pair_recv.at[j, kind - 1, k], me, pair
        )

    def spread(j, k):
        exchange(j, k).wait_recv()
        forward(j, k, 0).start()
        forward(j, k, 1).start()

    def fill(j, block):
        chosen = pick_ref[block]
        if j == 0:
            rows = jnp.dot(chosen, normed[...], preferred_element_type=jnp.float32)
        else:
            rows = jnp.dot(chosen, cot_ref[:, lanes(tp)], preferred_element_type=jnp.float32)
            rows = rows * weight_ref[block]
        ins[j][block] = rows.astype(jnp.bfloat16)

    def begin(j):
        fill(j, lax.rem(me + 1, n))

        def one(k):
            fill(j, lax.rem(me + k + 1, n))
            exchange(j, k).start()

        each(1, n, one)
        own(j).start()
        own(j).wait()
        forward(j, 0, 0).start()
        forward(j, 0, 1).start()

    def twin_done(j, k):
        block = lax.rem(me - k + n, n)
        forward(j, k, 0).wait_recv()
        forward(j, k, 2).start()

    half = n // 2
    carry.send(0)
    every = hidden_ref[...].astype(jnp.float32)
    row_scale = lax.rsqrt(jnp.mean(every * every, axis=-1, keepdims=True) + eps_value)
    mine = hidden_ref[:, lanes(tp)].astype(jnp.float32) * row_scale * gain_ref[:, lanes(tp)]
    normed[...] = mine.astype(jnp.bfloat16)
    begin(0)
    carry.receive(0, steps == 1)
    if steps > 1:
        carry.send(1)
    each(1, half, lambda k: spread(0, k))
    begin(1)
    each(half, n, lambda k: spread(0, k))
    for step in range(1, steps):
        carry.receive(step, step == steps - 1)
        if step + 1 < steps:
            carry.send(step + 1)
    each(1, half, lambda k: spread(1, k))
    each(0, n, lambda k: twin_done(0, k))
    each(half, n, lambda k: spread(1, k))
    each(0, n, lambda k: twin_done(1, k))
    carry.finish(steps)
    for j in range(2):
        each(1, n, lambda k: exchange(j, k).wait_send())

        def finish(k):
            forward(j, k, 0).wait_send()
            for kind in (1, 2):
                forward(j, k, kind).wait()

        each(0, n, finish)


def vmem(count):
    return [pl.BlockSpec(memory_space=pltpu.VMEM)] * count


def dispatch(n, hidden, cot, gain, pick, weight, packed):
    count, cap = pick.shape[:2]
    width = hidden.shape[1] // 4
    part = pltpu.VMEM((count, cap, width), jnp.bfloat16)
    full = jax.ShapeDtypeStruct((count, cap, 4 * width), jnp.bfloat16)
    dma = pltpu.SemaphoreType.DMA
    return pl.pallas_call(
        functools.partial(dispatch_kernel, n),
        out_shape=[full, full, jax.ShapeDtypeStruct(packed.shape, jnp.float32)],
        in_specs=vmem(6),
        out_specs=vmem(3),
        scratch_shapes=carry_scratch(n, packed.shape)
        + [
            part,
            part,
            pltpu.VMEM((hidden.shape[0], width), jnp.bfloat16),
            dma((2,)),
            dma((2, n)),
            dma((2, n)),
            dma((2, 2, n)),
            dma((2, 2, n)),
            dma((2, n)),
            dma((2, n)),
        ],
        compiler_params=pltpu.CompilerParams(
            collective_id=0, has_side_effects=True, vmem_limit_bytes=40 << 20
        ),
        name="dispatch",
    )(hidden, cot, gain, pick, weight, packed)


def return_kernel(
    n,
    part_ref,
    mix_ref,
    pick_ref,
    hidden_ref,
    cot_ref,
    gain_ref,
    w_ref,
    mixed_grad_out,
    mix_grad_out,
    mix_out,
    back_out,
    summed,
    features,
    mixed_grad,
    near,
    far_sum,
    far,
    total,
    local_sem,
    near_send,
    near_recv,
    far_send,
    far_recv,
    send_sem,
    recv_sem,
    mix_send,
    mix_recv,
    feature_send,
    feature_recv,
):
    me, tp = lax.axis_index("sp"), lax.axis_index("tp")
    pair, twin = tp_pair(tp)
    pair_twin = lax.rem(pair + 2, 4)
    width = back_out.shape[2]
    greet(n, me, tp, [(me, pair), (me, twin)])

    def lanes(t):
        return pl.ds(pl.multiple_of(t * width, 128), width)

    def to_pair(kind, k):
        block = lax.rem(me + k, n)
        return remote(
            part_ref.at[block, :, lanes(pair if kind == 0 else pair_twin)],
            near.at[kind, block],
            near_send.at[kind, k],
            near_recv.at[kind, k],
            me,
            pair,
        )

    def to_twin(k):
        block = lax.rem(me + k, n)
        return remote(far_sum.at[block], far.at[block], far_send.at[k], far_recv.at[k], me, twin)

    def to_owner(k):
        block = lax.rem(me + k, n)
        return remote(total.at[block], back_out.at[me], send_sem.at[k], recv_sem.at[k], block, tp)

    mix_steps = (n - 1).bit_length()

    def mixed(step, j, from_me):
        d = n >> (step + 1)
        other = me + d * (1 - 2 * lax.rem(lax.div(me, d), 2))
        block = lax.rem(me if from_me else other, 2 * d) + 2 * d * j
        piece = mix_out.at[block]
        return remote(piece, piece, mix_send.at[step, j], mix_recv.at[block], other, tp)

    def mix_start(step):
        each(0, 1 << step, lambda j: mixed(step, j, True).start())

    def mix_finish(step):
        each(0, 1 << step, lambda j: mixed(step, j, False).wait_recv())

    each(1, n + 1, lambda k: to_pair(1, lax.rem(k, n)).start())
    each(1, n + 1, lambda k: to_pair(0, lax.rem(k, n)).start())
    own_mix = pltpu.make_async_copy(mix_ref, mix_out.at[me], local_sem.at[0])
    own_mix.start()
    own_mix.wait()
    mix_start(0)

    def reduce_pair(i):
        k = lax.rem(i, n)
        block = lax.rem(me + k, n)
        to_pair(1, k).wait_recv()
        mine = part_ref[block, :, lanes(twin)].astype(jnp.float32)
        far_sum[block] = (mine + near[1, block].astype(jnp.float32)).astype(jnp.bfloat16)
        pl.when(i > 1)(lambda: to_twin(i - 1).start())

    each(1, n + 1, reduce_pair)
    to_twin(0).start()
    mix_finish(0)
    if mix_steps > 1:
        mix_start(1)

    def reduce_all(i):
        k = lax.rem(i, n)
        block = lax.rem(me + k, n)
        to_pair(0, k).wait_recv()
        to_twin(k).wait_recv()
        mine = part_ref[block, :, lanes(tp)].astype(jnp.float32)
        mine = mine + near[0, block].astype(jnp.float32) + far[block].astype(jnp.float32)
        total[block] = mine.astype(jnp.bfloat16)
        pl.when(i > 1)(lambda: to_owner(i - 1).start())

    each(1, n + 1, reduce_all)
    back_out[me] = total[me]
    if mix_steps > 1:
        mix_finish(1)
    for step in range(2, mix_steps):
        mix_start(step)
        if step + 1 < mix_steps:
            mix_finish(step)

    summed[...] = jnp.dot(pick_ref[me], back_out[me], preferred_element_type=jnp.float32)

    def gather(k):
        block = lax.rem(me - k + n, n)
        to_owner(k).wait_recv()
        summed[...] += jnp.dot(
            pick_ref[block], back_out[block], preferred_element_type=jnp.float32
        )

    each(1, n, gather)
    features[tp] = summed[...].astype(jnp.bfloat16)
    spread = [
        remote(
            features.at[q], features.at[q], feature_send.at[i], feature_recv.at[i], me, other
        )
        for i, (q, other) in enumerate([(tp, twin), (tp, pair), (twin, pair)])
    ]
    spread[0].start()
    spread[1].start()
    def finish(k):
        for kind in (0, 1):
            to_pair(kind, k).wait_send()
        to_twin(k).wait_send()

    each(0, n, finish)

    def finish_far(k):
        to_owner(k).wait_send()

    each(1, n, finish_far)
    if mix_steps > 2:
        mix_finish(mix_steps - 1)
    for step in range(mix_steps):
        each(0, 1 << step, lambda j, step=step: mixed(step, j, True).wait_send())
    spread[0].wait_recv()
    spread[2].start()
    spread[1].wait()
    spread[2].wait()
    spread[0].wait_send()
    rows = 32
    parts = mixed_grad_out.shape[0]

    def grads(i):
        here = pl.ds(pl.multiple_of(i * rows, rows), rows)
        state = hidden_ref[here, :].astype(jnp.float32)
        row_scale = lax.rsqrt(jnp.mean(state * state, axis=-1, keepdims=True) + eps_value)
        unit = state * row_scale
        back = jnp.concatenate([features[q, here, :] for q in range(4)], axis=1)
        grad = back.astype(jnp.float32) * gain_ref[...]
        grad = row_scale * (grad - unit * jnp.mean(grad * unit, axis=-1, keepdims=True))
        mixed_rows = (cot_ref[here, :].astype(jnp.float32) + grad).astype(jnp.bfloat16)
        mixed_grad[here, :] = mixed_rows
        piece = mixed_rows.shape[1] // parts
        for q in range(parts):
            mixed_grad_out[q, here, :] = mixed_rows[:, q * piece : (q + 1) * piece]

    each(0, hidden_ref.shape[0] // rows, grads)
    mix_grad_out[...] = jnp.dot(
        mixed_grad[...], w_ref[...], preferred_element_type=jnp.float32
    ).astype(jnp.bfloat16)


def give_back(n, partial_rows, mixed_out, pick, hidden, cot, gain, w_out):
    count, cap, model_width = partial_rows.shape
    tokens = hidden.shape[0]
    parts = n if (model_width // n) % 128 == 0 else 1
    width = model_width // 4
    dma = pltpu.SemaphoreType.DMA
    block = (count, cap, width)
    return pl.pallas_call(
        functools.partial(return_kernel, n),
        out_shape=[
            jax.ShapeDtypeStruct((parts, tokens, model_width // parts), jnp.bfloat16),
            jax.ShapeDtypeStruct(mixed_out.shape, jnp.bfloat16),
            jax.ShapeDtypeStruct((n,) + mixed_out.shape, jnp.bfloat16),
        ],
        in_specs=vmem(7),
        out_specs=vmem(3),
        scratch_shapes=[
            pltpu.VMEM(block, jnp.bfloat16),
            pltpu.VMEM((tokens, width), jnp.float32),
            pltpu.VMEM((4, tokens, width), jnp.bfloat16),
            pltpu.VMEM((tokens, model_width), jnp.bfloat16),
            pltpu.VMEM((2,) + block, jnp.bfloat16),
            pltpu.VMEM(block, jnp.bfloat16),
            pltpu.VMEM(block, jnp.bfloat16),
            pltpu.VMEM(block, jnp.bfloat16),
            dma((1,)),
            dma((2, n)),
            dma((2, n)),
            dma((n,)),
            dma((n,)),
            dma((n,)),
            dma((n,)),
            dma(((n - 1).bit_length(), max(1, n // 2))),
            dma((n,)),
            dma((3,)),
            dma((3,)),
        ],
        compiler_params=pltpu.CompilerParams(
            collective_id=1, has_side_effects=True, vmem_limit_bytes=40 << 20
        ),
        name="give_back",
    )(partial_rows, mixed_out, pick, hidden, cot, gain, w_out)


def last_kernel(
    n,
    rows_ref,
    state_ref,
    rows_out,
    scan_out,
    held,
    sent,
    carry_send,
    carry_recv,
    local_sem,
    send_sem,
    recv_sem,
    pair_send,
    pair_recv,
    twin_send,
    twin_recv,
):
    me, tp = lax.axis_index("sp"), lax.axis_index("tp")
    pair, twin = tp_pair(tp)
    greet(n, me, tp, [(me, pair), (me, twin)])
    share = rows_ref.shape[1] // 4

    def rows_of(t):
        return pl.ds(pl.multiple_of(t * share, share), share)

    steps = steps_of(n)
    carry = Carry(n, me, tp, True, state_ref, held, sent, scan_out, carry_send, carry_recv)

    def exchange(k):
        to = lax.rem(me + k, n)
        return remote(
            rows_ref.at[to, rows_of(tp)],
            rows_out.at[me, rows_of(tp)],
            send_sem.at[k],
            recv_sem.at[k],
            to,
            tp,
        )

    def forward(k, kind):
        block = lax.rem(me - k + n, n)
        piece = rows_out.at[block, rows_of(twin if kind == 2 else tp)]
        if kind == 0:
            return remote(piece, piece, twin_send.at[k], twin_recv.at[k], me, twin)
        return remote(piece, piece, pair_send.at[kind - 1, k], pair_recv.at[kind - 1, k], me, pair)

    def spread(k):
        exchange(k).wait_recv()
        forward(k, 0).start()
        forward(k, 1).start()

    def twin_done(k):
        forward(k, 0).wait_recv()
        forward(k, 2).start()

    def finish(k):
        exchange(k).wait_send()
        forward(k, 0).wait_send()
        forward(k, 1).wait()
        forward(k, 2).wait()

    own = pltpu.make_async_copy(rows_ref.at[me], rows_out.at[me], local_sem.at[0])
    carry.send(0)
    own.start()
    each(1, n, lambda k: exchange(k).start())
    for step in range(steps):
        carry.receive(step, step == steps - 1)
        if step + 1 < steps:
            carry.send(step + 1)
        if step == 0:
            each(1, n, spread)
    each(1, n, twin_done)
    carry.finish(steps)
    own.wait()
    each(1, n, finish)


def last_exchange(n, rows, packed):
    dma = pltpu.SemaphoreType.DMA
    return pl.pallas_call(
        functools.partial(last_kernel, n),
        out_shape=[
            jax.ShapeDtypeStruct(rows.shape, rows.dtype),
            jax.ShapeDtypeStruct(packed.shape, jnp.float32),
        ],
        in_specs=vmem(2),
        out_specs=vmem(2),
        scratch_shapes=carry_scratch(n, packed.shape) + [
            dma((1,)),
            dma((n,)),
            dma((n,)),
            dma((2, n)),
            dma((2, n)),
            dma((n,)),
            dma((n,)),
        ],
        compiler_params=pltpu.CompilerParams(
            collective_id=3, has_side_effects=True, vmem_limit_bytes=40 << 20
        ),
        name="last_exchange",
    )(rows, packed)


def pack_state(state, decay):
    heads, keys, values = state.shape
    rows = state.transpose(2, 0, 1).reshape(values, heads * keys)
    return jnp.concatenate([rows, jnp.broadcast_to(decay.reshape(1, -1), (8, heads * keys))], axis=0)


def unpack_state(packed, heads):
    rows = packed[:-8]
    return rows.reshape(rows.shape[0], heads, -1).transpose(1, 2, 0)


def carry_blocks(carried_state, inputs):
    decay_now, term_now = inputs
    return (decay_now[:, :, None] * carried_state + term_now, carried_state)


def block_scan(decays, terms, state, reverse):
    count = decays.shape[0]
    starts = [None] * count
    for i in reversed(range(count)) if reverse else range(count):
        state, starts[i] = carry_blocks(state, (decays[i], terms[i]))
    return state, jnp.stack(starts)


def body(
    hidden_state,
    norm_gain,
    route_ids,
    route_logits,
    cotangent,
    w_gate,
    w_up,
    w_down,
    w_out,
    query_rows,
    key_rows,
    value_rows,
    log_decay,
    head_gain,
):
    tok_count, model_width = hidden_state.shape
    head_count = head_gain.shape[0] // VAL_DIM
    block_count = tok_count // BLOCK
    shape_key = (block_count, BLOCK, head_count, KEY_DIM)
    shape_value = (block_count, BLOCK, head_count, VAL_DIM)
    query_f = query_rows.astype(jnp.float32).reshape(shape_key)
    key_f = key_rows.astype(jnp.float32).reshape(shape_key)
    value_f = value_rows.astype(jnp.float32).reshape(shape_value)
    cumulative_decay = jnp.cumsum(log_decay.reshape(shape_key), axis=1)
    decay_mid = cumulative_decay[:, BLOCK // 2 : BLOCK // 2 + 1]
    final_decay = cumulative_decay[:, BLOCK - 1 : BLOCK]
    query_in = query_f * jnp.exp(cumulative_decay - decay_mid)
    key_in = key_f * jnp.exp(decay_mid - cumulative_decay)
    key_end = key_f * jnp.exp(final_decay - cumulative_decay)
    query_start = query_f * jnp.exp(cumulative_decay)
    causal = (jnp.arange(BLOCK)[:, None] >= jnp.arange(BLOCK)[None, :])[None, None]
    last_logs = final_decay[:, 0]
    through = jnp.cumsum(last_logs, axis=0)
    total_log = through[-1]
    total_decay = jnp.exp(total_log)
    block_decay = jnp.exp(last_logs)
    block_kv = jnp.einsum("bshk,bshv->bhkv", key_end, value_f, precision=exact_numeric_mode)
    zero_state = jnp.zeros((head_count, KEY_DIM, VAL_DIM), jnp.float32)
    ones_decay = jnp.ones_like(total_log)
    local_end, local_start = block_scan(block_decay, block_kv, zero_state, False)
    sp_count = lax.axis_size("sp")
    route_weight = jax.nn.softmax(route_logits, axis=-1)
    expert_count = sp_count
    capacity = 4 * tok_count // expert_count
    named = route_ids[:, :, None] == jnp.arange(expert_count, dtype=jnp.int32)[None, None, :]
    names = jnp.any(named, axis=1)
    weight_of = jnp.sum(jnp.where(named, route_weight[:, :, None], 0.0), axis=1)
    before = (jnp.arange(tok_count)[:, None] > jnp.arange(tok_count)[None, :]).astype(jnp.bfloat16)
    rank = jnp.dot(before, names.astype(jnp.bfloat16), preferred_element_type=jnp.float32)
    place = jnp.where(names, rank, -1.0).T
    filled = place[:, None, :] == jnp.arange(capacity, dtype=jnp.float32)[None, :, None]
    slot_weight = jnp.sum(jnp.where(filled, weight_of.T[:, None, :], 0.0), axis=2)
    got_in, got_grad, scanned = dispatch(
        sp_count,
        hidden_state,
        cotangent,
        norm_gain.reshape(1, -1),
        filled.astype(jnp.bfloat16),
        slot_weight[:, :, None],
        pack_state(local_end, total_decay),
    )
    state_in = unpack_state(scanned, head_count)
    block_states = local_start + jnp.exp(through - last_logs)[:, :, :, None] * state_in
    end_state = total_decay[:, :, None] * state_in + local_end
    scores = jnp.where(
        causal, jnp.einsum("bthk,bshk->bhts", query_in, key_in, precision=exact_numeric_mode), 0.0
    )
    head_out = jnp.einsum("bhts,bshv->bthv", scores, value_f, precision=exact_numeric_mode)
    head_out = head_out + jnp.einsum(
        "bthk,bhkv->bthv", query_start, block_states, precision=exact_numeric_mode
    )
    inv_rms = lax.rsqrt(jnp.mean(head_out * head_out, axis=-1, keepdims=True) + eps_value)
    normed = head_out * inv_rms
    gain_heads = head_gain.reshape(head_count, VAL_DIM)
    mixed_out = (normed * gain_heads).reshape(tok_count, head_count * VAL_DIM).astype(jnp.bfloat16)
    rows_in = got_in.reshape(-1, model_width)
    rows_grad = got_grad.reshape(-1, model_width)
    gate_w = w_gate[0]
    up_w = w_up[0]
    down_w = w_down[0]
    gate_pre = jnp.dot(rows_in, gate_w, preferred_element_type=jnp.float32)
    up_pre = jnp.dot(rows_in, up_w, preferred_element_type=jnp.float32)
    gate_sig = jax.nn.sigmoid(gate_pre)
    silu_gate = gate_pre * gate_sig
    hidden_units = (silu_gate * up_pre).astype(jnp.bfloat16)
    grad_down = jnp.einsum("rf,rd->fd", hidden_units, rows_grad, preferred_element_type=jnp.float32)
    grad_hidden = jnp.einsum("rd,fd->rf", rows_grad, down_w, preferred_element_type=jnp.float32)
    grad_gate_pre = (grad_hidden * up_pre * gate_sig * (1.0 + gate_pre * (1.0 - gate_sig))).astype(
        jnp.bfloat16
    )
    grad_up_pre = (grad_hidden * silu_gate).astype(jnp.bfloat16)
    grad_gate_w = jnp.einsum(
        "rd,rf->df", rows_in, grad_gate_pre, preferred_element_type=jnp.float32
    )
    grad_up_w = jnp.einsum("rd,rf->df", rows_in, grad_up_pre, preferred_element_type=jnp.float32)
    partial_rows = jnp.einsum(
        "rf,df->rd", grad_gate_pre, gate_w, preferred_element_type=jnp.float32
    )
    partial_rows = partial_rows + jnp.einsum(
        "rf,df->rd", grad_up_pre, up_w, preferred_element_type=jnp.float32
    )
    partial_rows = partial_rows.reshape(expert_count, capacity, model_width)
    mixed_parts, grad_mix, mixed_all = give_back(
        sp_count,
        partial_rows.astype(jnp.bfloat16),
        mixed_out,
        (place[:, :, None] == jnp.arange(capacity, dtype=jnp.float32)).astype(jnp.bfloat16),
        hidden_state,
        cotangent,
        norm_gain.reshape(1, -1),
        w_out,
    )
    if mixed_parts.shape[0] != sp_count:
        mixed_parts = mixed_parts.reshape(tok_count, sp_count, -1).transpose(1, 0, 2)
    grad_mix = grad_mix.astype(jnp.float32).reshape(shape_value)
    grad_scaled = grad_mix * gain_heads
    grad_out = inv_rms * (
        grad_scaled - normed * jnp.mean(grad_scaled * normed, axis=-1, keepdims=True)
    )
    block_adj = jnp.einsum("bthk,bthv->bhkv", query_start, grad_out, precision=exact_numeric_mode)
    local_adj, later_adj = block_scan(block_decay, block_adj, zero_state, True)
    got_mixed, behind = last_exchange(sp_count, mixed_parts, pack_state(local_adj, total_decay))
    grad_out_w = jnp.einsum("ntd,nth->dh", got_mixed, mixed_all, preferred_element_type=jnp.float32)
    adj_end = unpack_state(behind, head_count)
    block_adj_end = later_adj + jnp.exp(total_log - through)[:, :, :, None] * adj_end
    grad_dots = jnp.where(
        causal, jnp.einsum("bthv,bshv->bhts", grad_out, value_f, precision=exact_numeric_mode), 0.0
    )
    grad_query = jnp.exp(cumulative_decay - decay_mid) * jnp.einsum(
        "bhts,bshk->bthk", grad_dots, key_in, precision=exact_numeric_mode
    )
    grad_query = grad_query + jnp.exp(cumulative_decay) * jnp.einsum(
        "bthv,bhkv->bthk", grad_out, block_states, precision=exact_numeric_mode
    )
    grad_key = jnp.exp(decay_mid - cumulative_decay) * jnp.einsum(
        "bhts,bthk->bshk", grad_dots, query_in, precision=exact_numeric_mode
    )
    grad_key = grad_key + jnp.exp(final_decay - cumulative_decay) * jnp.einsum(
        "bhkv,bshv->bshk", block_adj_end, value_f, precision=exact_numeric_mode
    )
    grad_value = jnp.einsum("bhts,bthv->bshv", scores, grad_out, precision=exact_numeric_mode)
    grad_value = grad_value + jnp.einsum(
        "bshk,bhkv->bshv", key_end, block_adj_end, precision=exact_numeric_mode
    )
    log_terms = (query_f * grad_query - key_f * grad_key).reshape(tok_count, head_count * KEY_DIM)
    suffix = lax.cumsum(log_terms, axis=0, reverse=True)
    tail_term = jnp.sum(adj_end * end_state, axis=-1).reshape(1, head_count * KEY_DIM)
    grad_log = suffix + tail_term
    return (
        grad_gate_w.astype(jnp.bfloat16)[None],
        grad_up_w.astype(jnp.bfloat16)[None],
        grad_down.astype(jnp.bfloat16)[None],
        grad_out_w,
        grad_query.reshape(tok_count, -1).astype(jnp.bfloat16),
        grad_key.reshape(tok_count, -1).astype(jnp.bfloat16),
        grad_value.reshape(tok_count, -1).astype(jnp.bfloat16),
        grad_log,
    )


def solution(mesh):
    in_specs = (
        P("sp", None),
        P(),
        P("sp", None),
        P("sp", None),
        P("sp", None),
        P("sp", None, "tp"),
        P("sp", None, "tp"),
        P("sp", "tp", None),
        P(None, "tp"),
        P("sp", "tp"),
        P("sp", "tp"),
        P("sp", "tp"),
        P("sp", "tp"),
        P("tp"),
    )
    out_specs = (
        P("sp", None, "tp"),
        P("sp", None, "tp"),
        P("sp", "tp", None),
        P("sp", "tp"),
        P("sp", "tp"),
        P("sp", "tp"),
        P("sp", "tp"),
        P("sp", "tp"),
    )
    return jax.shard_map(body, mesh=mesh, in_specs=in_specs, out_specs=out_specs, check_vma=False)
```

```python
import functools
import jax
import jax.numpy as jnp
from jax import lax
from jax.experimental import pallas as pl
from jax.experimental.pallas import tpu as pltpu
from jax.sharding import PartitionSpec as P

KEY_DIM = 64
VAL_DIM = 128
BLOCK = 64
MESH = pl.DeviceIdType.MESH


exact_numeric_mode = lax.Precision.HIGHEST
eps_value = 1e-06


def remote(src, dst, send, recv, sp, tp):
    return pltpu.make_async_remote_copy(
        src_ref=src, dst_ref=dst, send_sem=send, recv_sem=recv, device_id=(sp, tp), device_id_type=MESH
    )


def each(start, stop, step):
    lax.fori_loop(start, stop, lambda k, _: (step(k), 0)[1], 0)


def greet(n, me, tp, others):
    barrier = pltpu.get_barrier_semaphore()

    def hello(k):
        pl.semaphore_signal(
            barrier, inc=1, device_id=(lax.rem(me + k, n), tp), device_id_type=MESH
        )

    if n > 1:
        each(1, n, hello)
    for sp, other in others:
        pl.semaphore_signal(barrier, inc=1, device_id=(sp, other), device_id_type=MESH)
    pl.semaphore_wait(barrier, n - 1 + len(others))


class Carry:
    def __init__(self, n, me, tp, reverse, first, held, sent, scan, send_sem, recv_sem):
        self.n, self.me, self.tp, self.reverse = n, me, tp, reverse
        self.first, self.held, self.sent, self.scan = first, held, sent, scan
        self.send_sem, self.recv_sem = send_sem, recv_sem
        self.rows = first.shape[0] - 8
        self.scan[...] = jnp.zeros_like(self.scan)

    def parts(self, step):
        d = 1 << step
        n, me = self.n, self.me
        if self.reverse:
            to, has_to, has_from = lax.rem(me - d + n, n), me >= d, me + d < n
        else:
            to, has_to, has_from = lax.rem(me + d, n), me + d < n, me >= d
        src = self.first if step == 0 else self.sent.at[step - 1]
        copy = remote(
            src, self.held.at[step], self.send_sem.at[step], self.recv_sem.at[step], to, self.tp
        )
        return copy, has_to, has_from

    def send(self, step):
        copy, has_to, _ = self.parts(step)
        pl.when(has_to)(lambda: copy.start())

    def receive(self, step, last):
        copy, _, has_from = self.parts(step)
        rows = self.rows
        now = self.first if step == 0 else self.sent.at[step - 1]

        @pl.when(has_from)
        def _():
            copy.wait_recv()

        if not last:

            @pl.when(has_from)
            def _():
                other = self.held[step]
                mine = now[...]
                self.sent[step] = mine[rows : rows + 1] * other
                self.sent[step, :rows] += mine[:rows]

            @pl.when(jnp.logical_not(has_from))
            def _():
                self.sent[step] = now[...]

        @pl.when(has_from)
        def _():
            other = self.held[step]
            if step == 0:
                self.scan[...] = other
            else:
                mine = self.scan[...]
                self.scan[...] = mine[rows : rows + 1] * other
                self.scan[:rows, :] += mine[:rows]

    def finish(self, steps):
        for step in range(steps):
            copy, has_to, _ = self.parts(step)
            pl.when(has_to)(lambda copy=copy: copy.wait_send())


def steps_of(n):
    return max(1, (n - 1).bit_length())


def carry_scratch(n, shape):
    steps = steps_of(n)
    return [
        pltpu.VMEM((steps,) + shape, jnp.float32),
        pltpu.VMEM((steps,) + shape, jnp.float32),
        pltpu.SemaphoreType.DMA((steps,)),
        pltpu.SemaphoreType.DMA((steps,)),
    ]


def tp_pair(tp):
    return tp + 1 - 2 * lax.rem(tp, 2), lax.rem(tp + 2, 4)


def dispatch_kernel(
    n,
    hidden_ref,
    cot_ref,
    gain_ref,
    pick_ref,
    weight_ref,
    state_ref,
    a_out,
    b_out,
    scan_out,
    held,
    sent,
    carry_send,
    carry_recv,
    a_ref,
    b_ref,
    normed,
    local_sem,
    send_sem,
    recv_sem,
    pair_send,
    pair_recv,
    twin_send,
    twin_recv,
):
    me, tp = lax.axis_index("sp"), lax.axis_index("tp")
    pair, twin = tp_pair(tp)
    width = a_ref.shape[2]
    greet(n, me, tp, [(me, pair), (me, twin)])
    steps = steps_of(n)
    carry = Carry(n, me, tp, False, state_ref, held, sent, scan_out, carry_send, carry_recv)
    ins, outs = (a_ref, b_ref), (a_out, b_out)

    def lanes(t):
        return pl.ds(pl.multiple_of(t * width, 128), width)

    def exchange(j, k):
        to = lax.rem(me + k, n)
        return remote(
            ins[j].at[to],
            outs[j].at[me, :, lanes(tp)],
            send_sem.at[j, k],
            recv_sem.at[j, k],
            to,
            tp,
        )

    def own(j):
        return pltpu.make_async_copy(
            ins[j].at[me], outs[j].at[me, :, lanes(tp)], local_sem.at[j]
        )

    def forward(j, k, kind):
        block = lax.rem(me - k + n, n)
        if kind == 0:
            piece = outs[j].at[block, :, lanes(tp)]
            return remote(
                piece, piece, twin_send.at[j, k], twin_recv.at[j, k], me, twin
            )
        piece = outs[j].at[block, :, lanes(tp if kind == 1 else twin)]
        return remote(
            piece, piece, pair_send.at[j, kind - 1, k], pair_recv.at[j, kind - 1, k], me, pair
        )

    def spread(j, k):
        exchange(j, k).wait_recv()
        forward(j, k, 0).start()
        forward(j, k, 1).start()

    def fill(j, block):
        chosen = pick_ref[block]
        if j == 0:
            rows = jnp.dot(chosen, normed[...], preferred_element_type=jnp.float32)
        else:
            rows = jnp.dot(chosen, cot_ref[:, lanes(tp)], preferred_element_type=jnp.float32)
            rows = rows * weight_ref[block]
        ins[j][block] = rows.astype(jnp.bfloat16)

    def begin(j):
        fill(j, lax.rem(me + 1, n))

        def one(k):
            fill(j, lax.rem(me + k + 1, n))
            exchange(j, k).start()

        each(1, n, one)
        own(j).start()
        own(j).wait()
        forward(j, 0, 0).start()
        forward(j, 0, 1).start()

    def twin_done(j, k):
        block = lax.rem(me - k + n, n)
        forward(j, k, 0).wait_recv()
        forward(j, k, 2).start()

    half = n // 2
    carry.send(0)
    every = hidden_ref[...].astype(jnp.float32)
    row_scale = lax.rsqrt(jnp.mean(every * every, axis=-1, keepdims=True) + eps_value)
    mine = hidden_ref[:, lanes(tp)].astype(jnp.float32) * row_scale * gain_ref[:, lanes(tp)]
    normed[...] = mine.astype(jnp.bfloat16)
    begin(0)
    carry.receive(0, steps == 1)
    if steps > 1:
        carry.send(1)
    each(1, half, lambda k: spread(0, k))
    begin(1)
    each(half, n, lambda k: spread(0, k))
    for step in range(1, steps):
        carry.receive(step, step == steps - 1)
        if step + 1 < steps:
            carry.send(step + 1)
    each(1, half, lambda k: spread(1, k))
    each(0, n, lambda k: twin_done(0, k))
    each(half, n, lambda k: spread(1, k))
    each(0, n, lambda k: twin_done(1, k))
    carry.finish(steps)
    for j in range(2):
        each(1, n, lambda k: exchange(j, k).wait_send())

        def finish(k):
            forward(j, k, 0).wait_send()
            for kind in (1, 2):
                forward(j, k, kind).wait()

        each(0, n, finish)


def vmem(count):
    return [pl.BlockSpec(memory_space=pltpu.VMEM)] * count


def dispatch(n, hidden, cot, gain, pick, weight, packed):
    count, cap = pick.shape[:2]
    width = hidden.shape[1] // 4
    part = pltpu.VMEM((count, cap, width), jnp.bfloat16)
    full = jax.ShapeDtypeStruct((count, cap, 4 * width), jnp.bfloat16)
    dma = pltpu.SemaphoreType.DMA
    return pl.pallas_call(
        functools.partial(dispatch_kernel, n),
        out_shape=[full, full, jax.ShapeDtypeStruct(packed.shape, jnp.float32)],
        in_specs=vmem(6),
        out_specs=vmem(3),
        scratch_shapes=carry_scratch(n, packed.shape)
        + [
            part,
            part,
            pltpu.VMEM((hidden.shape[0], width), jnp.bfloat16),
            dma((2,)),
            dma((2, n)),
            dma((2, n)),
            dma((2, 2, n)),
            dma((2, 2, n)),
            dma((2, n)),
            dma((2, n)),
        ],
        compiler_params=pltpu.CompilerParams(
            collective_id=0, has_side_effects=True, vmem_limit_bytes=40 << 20
        ),
        name="dispatch",
    )(hidden, cot, gain, pick, weight, packed)


def return_kernel(
    n,
    part_ref,
    mix_ref,
    pick_ref,
    hidden_ref,
    cot_ref,
    gain_ref,
    w_ref,
    mixed_grad_out,
    mix_grad_out,
    mix_out,
    back_out,
    summed,
    features,
    mixed_grad,
    near,
    far_sum,
    far,
    total,
    local_sem,
    near_send,
    near_recv,
    far_send,
    far_recv,
    send_sem,
    recv_sem,
    mix_send,
    mix_recv,
    feature_send,
    feature_recv,
):
    me, tp = lax.axis_index("sp"), lax.axis_index("tp")
    pair, twin = tp_pair(tp)
    pair_twin = lax.rem(pair + 2, 4)
    width = back_out.shape[2]
    greet(n, me, tp, [(me, pair), (me, twin)])

    def lanes(t):
        return pl.ds(pl.multiple_of(t * width, 128), width)

    def to_pair(kind, k):
        block = lax.rem(me + k, n)
        return remote(
            part_ref.at[block, :, lanes(pair if kind == 0 else pair_twin)],
            near.at[kind, block],
            near_send.at[kind, k],
            near_recv.at[kind, k],
            me,
            pair,
        )

    def to_twin(k):
        block = lax.rem(me + k, n)
        return remote(far_sum.at[block], far.at[block], far_send.at[k], far_recv.at[k], me, twin)

    def to_owner(k):
        block = lax.rem(me + k, n)
        return remote(total.at[block], back_out.at[me], send_sem.at[k], recv_sem.at[k], block, tp)

    mix_steps = (n - 1).bit_length()

    def mixed(step, j, from_me):
        d = n >> (step + 1)
        other = me + d * (1 - 2 * lax.rem(lax.div(me, d), 2))
        block = lax.rem(me if from_me else other, 2 * d) + 2 * d * j
        piece = mix_out.at[block]
        return remote(piece, piece, mix_send.at[step, j], mix_recv.at[block], other, tp)

    def mix_start(step):
        each(0, 1 << step, lambda j: mixed(step, j, True).start())

    def mix_finish(step):
        each(0, 1 << step, lambda j: mixed(step, j, False).wait_recv())

    each(1, n + 1, lambda k: to_pair(1, lax.rem(k, n)).start())
    each(1, n + 1, lambda k: to_pair(0, lax.rem(k, n)).start())
    own_mix = pltpu.make_async_copy(mix_ref, mix_out.at[me], local_sem.at[0])
    own_mix.start()
    own_mix.wait()
    mix_start(0)

    def reduce_pair(i):
        k = lax.rem(i, n)
        block = lax.rem(me + k, n)
        to_pair(1, k).wait_recv()
        mine = part_ref[block, :, lanes(twin)].astype(jnp.float32)
        far_sum[block] = (mine + near[1, block].astype(jnp.float32)).astype(jnp.bfloat16)
        pl.when(i > 1)(lambda: to_twin(i - 1).start())

    each(1, n + 1, reduce_pair)
    to_twin(0).start()
    mix_finish(0)
    if mix_steps > 1:
        mix_start(1)

    def reduce_all(i):
        k = lax.rem(i, n)
        block = lax.rem(me + k, n)
        to_pair(0, k).wait_recv()
        to_twin(k).wait_recv()
        mine = part_ref[block, :, lanes(tp)].astype(jnp.float32)
        mine = mine + near[0, block].astype(jnp.float32) + far[block].astype(jnp.float32)
        total[block] = mine.astype(jnp.bfloat16)
        pl.when(i > 1)(lambda: to_owner(i - 1).start())

    each(1, n + 1, reduce_all)
    back_out[me] = total[me]
    if mix_steps > 1:
        mix_finish(1)
    for step in range(2, mix_steps):
        mix_start(step)
        if step + 1 < mix_steps:
            mix_finish(step)

    summed[...] = jnp.dot(pick_ref[me], back_out[me], preferred_element_type=jnp.float32)

    def gather(k):
        block = lax.rem(me - k + n, n)
        to_owner(k).wait_recv()
        summed[...] += jnp.dot(
            pick_ref[block], back_out[block], preferred_element_type=jnp.float32
        )

    each(1, n, gather)
    features[tp] = summed[...].astype(jnp.bfloat16)
    spread = [
        remote(
            features.at[q], features.at[q], feature_send.at[i], feature_recv.at[i], me, other
        )
        for i, (q, other) in enumerate([(tp, twin), (tp, pair), (twin, pair)])
    ]
    spread[0].start()
    spread[1].start()
    def finish(k):
        for kind in (0, 1):
            to_pair(kind, k).wait_send()
        to_twin(k).wait_send()

    each(0, n, finish)

    def finish_far(k):
        to_owner(k).wait_send()

    each(1, n, finish_far)
    if mix_steps > 2:
        mix_finish(mix_steps - 1)
    for step in range(mix_steps):
        each(0, 1 << step, lambda j, step=step: mixed(step, j, True).wait_send())
    spread[0].wait_recv()
    spread[2].start()
    spread[1].wait()
    spread[2].wait()
    spread[0].wait_send()
    rows = 32
    parts = mixed_grad_out.shape[0]

    def grads(i):
        here = pl.ds(pl.multiple_of(i * rows, rows), rows)
        state = hidden_ref[here, :].astype(jnp.float32)
        row_scale = lax.rsqrt(jnp.mean(state * state, axis=-1, keepdims=True) + eps_value)
        unit = state * row_scale
        back = jnp.concatenate([features[q, here, :] for q in range(4)], axis=1)
        grad = back.astype(jnp.float32) * gain_ref[...]
        grad = row_scale * (grad - unit * jnp.mean(grad * unit, axis=-1, keepdims=True))
        mixed_rows = (cot_ref[here, :].astype(jnp.float32) + grad).astype(jnp.bfloat16)
        mixed_grad[here, :] = mixed_rows
        piece = mixed_rows.shape[1] // parts
        for q in range(parts):
            mixed_grad_out[q, here, :] = mixed_rows[:, q * piece : (q + 1) * piece]

    each(0, hidden_ref.shape[0] // rows, grads)
    mix_grad_out[...] = jnp.dot(
        mixed_grad[...], w_ref[...], preferred_element_type=jnp.float32
    ).astype(jnp.bfloat16)


def give_back(n, partial_rows, mixed_out, pick, hidden, cot, gain, w_out):
    count, cap, model_width = partial_rows.shape
    tokens = hidden.shape[0]
    parts = n if (model_width // n) % 128 == 0 else 1
    width = model_width // 4
    dma = pltpu.SemaphoreType.DMA
    block = (count, cap, width)
    return pl.pallas_call(
        functools.partial(return_kernel, n),
        out_shape=[
            jax.ShapeDtypeStruct((parts, tokens, model_width // parts), jnp.bfloat16),
            jax.ShapeDtypeStruct(mixed_out.shape, jnp.bfloat16),
            jax.ShapeDtypeStruct((n,) + mixed_out.shape, jnp.bfloat16),
        ],
        in_specs=vmem(7),
        out_specs=vmem(3),
        scratch_shapes=[
            pltpu.VMEM(block, jnp.bfloat16),
            pltpu.VMEM((tokens, width), jnp.float32),
            pltpu.VMEM((4, tokens, width), jnp.bfloat16),
            pltpu.VMEM((tokens, model_width), jnp.bfloat16),
            pltpu.VMEM((2,) + block, jnp.bfloat16),
            pltpu.VMEM(block, jnp.bfloat16),
            pltpu.VMEM(block, jnp.bfloat16),
            pltpu.VMEM(block, jnp.bfloat16),
            dma((1,)),
            dma((2, n)),
            dma((2, n)),
            dma((n,)),
            dma((n,)),
            dma((n,)),
            dma((n,)),
            dma(((n - 1).bit_length(), max(1, n // 2))),
            dma((n,)),
            dma((3,)),
            dma((3,)),
        ],
        compiler_params=pltpu.CompilerParams(
            collective_id=1, has_side_effects=True, vmem_limit_bytes=40 << 20
        ),
        name="give_back",
    )(partial_rows, mixed_out, pick, hidden, cot, gain, w_out)


def last_kernel(
    n,
    rows_ref,
    state_ref,
    rows_out,
    scan_out,
    held,
    sent,
    carry_send,
    carry_recv,
    local_sem,
    send_sem,
    recv_sem,
    pair_send,
    pair_recv,
    twin_send,
    twin_recv,
):
    me, tp = lax.axis_index("sp"), lax.axis_index("tp")
    pair, twin = tp_pair(tp)
    greet(n, me, tp, [(me, pair), (me, twin)])
    share = rows_ref.shape[1] // 4

    def rows_of(t):
        return pl.ds(pl.multiple_of(t * share, share), share)

    steps = steps_of(n)
    carry = Carry(n, me, tp, True, state_ref, held, sent, scan_out, carry_send, carry_recv)

    def exchange(k):
        to = lax.rem(me + k, n)
        return remote(
            rows_ref.at[to, rows_of(tp)],
            rows_out.at[me, rows_of(tp)],
            send_sem.at[k],
            recv_sem.at[k],
            to,
            tp,
        )

    def forward(k, kind):
        block = lax.rem(me - k + n, n)
        piece = rows_out.at[block, rows_of(twin if kind == 2 else tp)]
        if kind == 0:
            return remote(piece, piece, twin_send.at[k], twin_recv.at[k], me, twin)
        return remote(piece, piece, pair_send.at[kind - 1, k], pair_recv.at[kind - 1, k], me, pair)

    def spread(k):
        exchange(k).wait_recv()
        forward(k, 0).start()
        forward(k, 1).start()

    def twin_done(k):
        forward(k, 0).wait_recv()
        forward(k, 2).start()

    def finish(k):
        exchange(k).wait_send()
        forward(k, 0).wait_send()
        forward(k, 1).wait()
        forward(k, 2).wait()

    own = pltpu.make_async_copy(rows_ref.at[me], rows_out.at[me], local_sem.at[0])
    carry.send(0)
    own.start()
    each(1, n, lambda k: exchange(k).start())
    for step in range(steps):
        carry.receive(step, step == steps - 1)
        if step + 1 < steps:
            carry.send(step + 1)
        if step == 0:
            each(1, n, spread)
    each(1, n, twin_done)
    carry.finish(steps)
    own.wait()
    each(1, n, finish)


def last_exchange(n, rows, packed):
    dma = pltpu.SemaphoreType.DMA
    return pl.pallas_call(
        functools.partial(last_kernel, n),
        out_shape=[
            jax.ShapeDtypeStruct(rows.shape, rows.dtype),
            jax.ShapeDtypeStruct(packed.shape, jnp.float32),
        ],
        in_specs=vmem(2),
        out_specs=vmem(2),
        scratch_shapes=carry_scratch(n, packed.shape) + [
            dma((1,)),
            dma((n,)),
            dma((n,)),
            dma((2, n)),
            dma((2, n)),
            dma((n,)),
            dma((n,)),
        ],
        compiler_params=pltpu.CompilerParams(
            collective_id=3, has_side_effects=True, vmem_limit_bytes=40 << 20
        ),
        name="last_exchange",
    )(rows, packed)


def pack_state(state, decay):
    heads, keys, values = state.shape
    rows = state.transpose(2, 0, 1).reshape(values, heads * keys)
    return jnp.concatenate([rows, jnp.broadcast_to(decay.reshape(1, -1), (8, heads * keys))], axis=0)


def unpack_state(packed, heads):
    rows = packed[:-8]
    return rows.reshape(rows.shape[0], heads, -1).transpose(1, 2, 0)


def carry_blocks(carried_state, inputs):
    decay_now, term_now = inputs
    return (decay_now[:, :, None] * carried_state + term_now, carried_state)


def block_scan(decays, terms, state, reverse):
    count = decays.shape[0]
    starts = [None] * count
    for i in reversed(range(count)) if reverse else range(count):
        state, starts[i] = carry_blocks(state, (decays[i], terms[i]))
    return state, jnp.stack(starts)


def body(
    hidden_state,
    norm_gain,
    route_ids,
    route_logits,
    cotangent,
    w_gate,
    w_up,
    w_down,
    w_out,
    query_rows,
    key_rows,
    value_rows,
    log_decay,
    head_gain,
):
    tok_count, model_width = hidden_state.shape
    head_count = head_gain.shape[0] // VAL_DIM
    block_count = tok_count // BLOCK
    shape_key = (block_count, BLOCK, head_count, KEY_DIM)
    shape_value = (block_count, BLOCK, head_count, VAL_DIM)
    query_f = query_rows.astype(jnp.float32).reshape(shape_key)
    key_f = key_rows.astype(jnp.float32).reshape(shape_key)
    value_f = value_rows.astype(jnp.float32).reshape(shape_value)
    cumulative_decay = jnp.cumsum(log_decay.reshape(shape_key), axis=1)
    decay_mid = cumulative_decay[:, BLOCK // 2 : BLOCK // 2 + 1]
    final_decay = cumulative_decay[:, BLOCK - 1 : BLOCK]
    query_in = query_f * jnp.exp(cumulative_decay - decay_mid)
    key_in = key_f * jnp.exp(decay_mid - cumulative_decay)
    key_end = key_f * jnp.exp(final_decay - cumulative_decay)
    query_start = query_f * jnp.exp(cumulative_decay)
    causal = (jnp.arange(BLOCK)[:, None] >= jnp.arange(BLOCK)[None, :])[None, None]
    last_logs = final_decay[:, 0]
    through = jnp.cumsum(last_logs, axis=0)
    total_log = through[-1]
    total_decay = jnp.exp(total_log)
    block_decay = jnp.exp(last_logs)
    block_kv = jnp.einsum("bshk,bshv->bhkv", key_end, value_f, precision=exact_numeric_mode)
    zero_state = jnp.zeros((head_count, KEY_DIM, VAL_DIM), jnp.float32)
    ones_decay = jnp.ones_like(total_log)
    local_end, local_start = block_scan(block_decay, block_kv, zero_state, False)
    sp_count = lax.axis_size("sp")
    expert_count = sp_count
    capacity = 4 * tok_count // expert_count
    experts = jnp.arange(expert_count, dtype=jnp.int32)[None, :]
    first, second = route_ids[:, :1] == experts, route_ids[:, 1:] == experts
    names = first | second
    margin = route_logits[:, :1] - route_logits[:, 1:]
    weight_of = jnp.where(first, margin, jnp.where(second, -margin, 0.0))
    weight_of = jnp.where(names, jax.nn.sigmoid(weight_of), 0.0)
    before = (jnp.arange(tok_count)[:, None] > jnp.arange(tok_count)[None, :]).astype(jnp.bfloat16)
    rank = jnp.dot(before, names.astype(jnp.bfloat16), preferred_element_type=jnp.float32)
    place = jnp.where(names, rank, -1.0).T
    filled = place[:, None, :] == jnp.arange(capacity, dtype=jnp.float32)[None, :, None]
    slot_weight = jnp.sum(jnp.where(filled, weight_of.T[:, None, :], 0.0), axis=2)
    got_in, got_grad, scanned = dispatch(
        sp_count,
        hidden_state,
        cotangent,
        norm_gain.reshape(1, -1),
        filled.astype(jnp.bfloat16),
        slot_weight[:, :, None],
        pack_state(local_end, total_decay),
    )
    state_in = unpack_state(scanned, head_count)
    block_states = local_start + jnp.exp(through - last_logs)[:, :, :, None] * state_in
    end_state = total_decay[:, :, None] * state_in + local_end
    scores = jnp.where(
        causal, jnp.einsum("bthk,bshk->bhts", query_in, key_in, precision=exact_numeric_mode), 0.0
    )
    head_out = jnp.einsum("bhts,bshv->bthv", scores, value_f, precision=exact_numeric_mode)
    head_out = head_out + jnp.einsum(
        "bthk,bhkv->bthv", query_start, block_states, precision=exact_numeric_mode
    )
    inv_rms = lax.rsqrt(jnp.mean(head_out * head_out, axis=-1, keepdims=True) + eps_value)
    normed = head_out * inv_rms
    gain_heads = head_gain.reshape(head_count, VAL_DIM)
    mixed_out = (normed * gain_heads).reshape(tok_count, head_count * VAL_DIM).astype(jnp.bfloat16)
    rows_in = got_in.reshape(-1, model_width)
    rows_grad = got_grad.reshape(-1, model_width)
    gate_w = w_gate[0]
    up_w = w_up[0]
    down_w = w_down[0]
    gate_pre = jnp.dot(rows_in, gate_w, preferred_element_type=jnp.float32)
    up_pre = jnp.dot(rows_in, up_w, preferred_element_type=jnp.float32)
    gate_sig = jax.nn.sigmoid(gate_pre)
    silu_gate = gate_pre * gate_sig
    hidden_units = (silu_gate * up_pre).astype(jnp.bfloat16)
    grad_down = jnp.einsum("rf,rd->fd", hidden_units, rows_grad, preferred_element_type=jnp.float32)
    grad_hidden = jnp.einsum("rd,fd->rf", rows_grad, down_w, preferred_element_type=jnp.float32)
    grad_gate_pre = (grad_hidden * up_pre * gate_sig * (1.0 + gate_pre * (1.0 - gate_sig))).astype(
        jnp.bfloat16
    )
    grad_up_pre = (grad_hidden * silu_gate).astype(jnp.bfloat16)
    grad_gate_w = jnp.einsum(
        "rd,rf->df", rows_in, grad_gate_pre, preferred_element_type=jnp.float32
    )
    grad_up_w = jnp.einsum("rd,rf->df", rows_in, grad_up_pre, preferred_element_type=jnp.float32)
    partial_rows = jnp.einsum(
        "rf,df->rd", grad_gate_pre, gate_w, preferred_element_type=jnp.float32
    )
    partial_rows = partial_rows + jnp.einsum(
        "rf,df->rd", grad_up_pre, up_w, preferred_element_type=jnp.float32
    )
    partial_rows = partial_rows.reshape(expert_count, capacity, model_width)
    mixed_parts, grad_mix, mixed_all = give_back(
        sp_count,
        partial_rows.astype(jnp.bfloat16),
        mixed_out,
        (place[:, :, None] == jnp.arange(capacity, dtype=jnp.float32)).astype(jnp.bfloat16),
        hidden_state,
        cotangent,
        norm_gain.reshape(1, -1),
        w_out,
    )
    if mixed_parts.shape[0] != sp_count:
        mixed_parts = mixed_parts.reshape(tok_count, sp_count, -1).transpose(1, 0, 2)
    grad_mix = grad_mix.astype(jnp.float32).reshape(shape_value)
    grad_scaled = grad_mix * gain_heads
    grad_out = inv_rms * (
        grad_scaled - normed * jnp.mean(grad_scaled * normed, axis=-1, keepdims=True)
    )
    block_adj = jnp.einsum("bthk,bthv->bhkv", query_start, grad_out, precision=exact_numeric_mode)
    local_adj, later_adj = block_scan(block_decay, block_adj, zero_state, True)
    got_mixed, behind = last_exchange(sp_count, mixed_parts, pack_state(local_adj, total_decay))
    grad_out_w = jnp.einsum("ntd,nth->dh", got_mixed, mixed_all, preferred_element_type=jnp.float32)
    adj_end = unpack_state(behind, head_count)
    block_adj_end = later_adj + jnp.exp(total_log - through)[:, :, :, None] * adj_end
    grad_dots = jnp.where(
        causal, jnp.einsum("bthv,bshv->bhts", grad_out, value_f, precision=exact_numeric_mode), 0.0
    )
    grad_query = jnp.exp(cumulative_decay - decay_mid) * jnp.einsum(
        "bhts,bshk->bthk", grad_dots, key_in, precision=exact_numeric_mode
    )
    grad_query = grad_query + jnp.exp(cumulative_decay) * jnp.einsum(
        "bthv,bhkv->bthk", grad_out, block_states, precision=exact_numeric_mode
    )
    grad_key = jnp.exp(decay_mid - cumulative_decay) * jnp.einsum(
        "bhts,bthk->bshk", grad_dots, query_in, precision=exact_numeric_mode
    )
    grad_key = grad_key + jnp.exp(final_decay - cumulative_decay) * jnp.einsum(
        "bhkv,bshv->bshk", block_adj_end, value_f, precision=exact_numeric_mode
    )
    grad_value = jnp.einsum("bhts,bthv->bshv", scores, grad_out, precision=exact_numeric_mode)
    grad_value = grad_value + jnp.einsum(
        "bshk,bhkv->bshv", key_end, block_adj_end, precision=exact_numeric_mode
    )
    log_terms = (query_f * grad_query - key_f * grad_key).reshape(tok_count, head_count * KEY_DIM)
    suffix = lax.cumsum(log_terms, axis=0, reverse=True)
    tail_term = jnp.sum(adj_end * end_state, axis=-1).reshape(1, head_count * KEY_DIM)
    grad_log = suffix + tail_term
    return (
        grad_gate_w.astype(jnp.bfloat16)[None],
        grad_up_w.astype(jnp.bfloat16)[None],
        grad_down.astype(jnp.bfloat16)[None],
        grad_out_w,
        grad_query.reshape(tok_count, -1).astype(jnp.bfloat16),
        grad_key.reshape(tok_count, -1).astype(jnp.bfloat16),
        grad_value.reshape(tok_count, -1).astype(jnp.bfloat16),
        grad_log,
    )


def solution(mesh):
    in_specs = (
        P("sp", None),
        P(),
        P("sp", None),
        P("sp", None),
        P("sp", None),
        P("sp", None, "tp"),
        P("sp", None, "tp"),
        P("sp", "tp", None),
        P(None, "tp"),
        P("sp", "tp"),
        P("sp", "tp"),
        P("sp", "tp"),
        P("sp", "tp"),
        P("tp"),
    )
    out_specs = (
        P("sp", None, "tp"),
        P("sp", None, "tp"),
        P("sp", "tp", None),
        P("sp", "tp"),
        P("sp", "tp"),
        P("sp", "tp"),
        P("sp", "tp"),
        P("sp", "tp"),
    )
    return jax.shard_map(body, mesh=mesh, in_specs=in_specs, out_specs=out_specs, check_vma=False)
```
